256 devices in a mesh: gr: 2 (over z_hi), sp: 16 (over z_lo, y), tp: 8 (over x, core).
Axes of the slice: x: 4, y: 4, z: 8 (z_hi: 2, z_lo: 4; z = z_hi * 4 + z_lo), core: 2. Of those that a mesh axis runs over, the one named last changes fastest.
Arguments:
- tokens: bfloat16 [8, 3072, 4096], P('gr', 'sp', 'tp'), may hold values from -6.5 to 6.5
- first_token_input: bfloat16 [8, 4096], P('gr', 'sp'), may hold values from -6 to 6
- forget_weight: bfloat16 [4096, 4096], P(None, 'tp'), may hold values from -0.1171875 to 0.1171875
- value_weight: bfloat16 [4096, 4096], P(None, 'tp'), may hold values from -0.375 to 0.375
- query_weight: bfloat16 [4096, 4096], P('sp', 'tp'), may hold values from -0.09375 to 0.09375
- output_gate_weight: bfloat16 [4096, 4096], P('sp', 'tp'), may hold values from -0.09375 to 0.09375
- forget_bound_slack: float32 [4096], P('tp'), may hold values from 0.00016276042 to 0.8, as said below
- additional_damping_exponent: float32 [8, 3072, 32], P('gr', 'sp', 'tp'), may hold values from -2.2 to 0, as said below
- read_norm_scale: float32 [128], replicated, may hold values from 0.1 to 1.9
Outputs:
- cache: bfloat16 [8, 32, 128, 128], P('gr', 'tp', 'sp')
- first_read: bfloat16 [8, 4096], P('gr', 'tp')
The draws below stay inside these ranges and needn't reach their ends.
Inputs may be any that keep to these rules, and one draw needn't show every extreme that they name: `forget_bound_slack`: positive gaps, one per channel. `additional_damping_exponent`: non-positive log-decays.
All inputs are finite; a program needn't handle non-finite values.
Results may differ from the reference program's by a relative error of at most 0.018.
Values may be sent and summed in bfloat16 or wider, within the bound.
No kernel may reach another device: no remote copies, remote signals or barrier semaphores. Data moves between devices by JAX's collectives and lax.ppermute only.
A program may use at most 64 MiB of HBM per device.

```python
import math
import jax
import jax.numpy as jnp
from jax import lax

D = 4096
HEADS = 32
ATTENTION_SPAN = 128
HW = 4096
LEN = 3072
SEQS_ALL = 8


def shared_direction(key):
    signs = jax.random.randint(jax.random.fold_in(key, 101), (D,), 0, 2)
    return (signs * 2 - 1).astype(jnp.float32)


def draw_tokens(key, part):
    direction = shared_direction(key)
    base_key, coef_key = jax.random.split(jax.random.fold_in(key, 31))
    base = jnp.clip(jax.random.normal(base_key, (SEQS_ALL, LEN, D), jnp.float32), -6.0, 6.0)
    coef = jax.random.uniform(coef_key, (SEQS_ALL, 16, 1), jnp.float32, 0.0, 1.5)
    coef = jnp.repeat(coef, LEN // 16, axis=1)
    return (base + coef * 0.3 * direction[None, None, :]).astype(jnp.bfloat16)


def draw_forget_weight(key, part):
    direction = shared_direction(key)
    base_key = jax.random.fold_in(key, 43)
    spread = 1.0 / math.sqrt(D)
    base = jnp.clip(jax.random.normal(base_key, (D, HW), jnp.float32), -6.0, 6.0) * spread
    return (base + 11.0 / D * direction[:, None]).astype(jnp.bfloat16)


def draw_forget_bound_slack(key, part):
    heads_key, jitter_key = jax.random.split(jax.random.fold_in(key, 11))
    share = 0.5
    slow = jax.random.uniform(heads_key, (HEADS,), jnp.float32) < share
    quick = min(0.4, max(0.05, 16.0 / LEN))
    base = jnp.where(slow, 1.0 / LEN, quick)
    jitter = jnp.exp(jax.random.uniform(jitter_key, (HEADS, ATTENTION_SPAN), jnp.float32, -0.69, 0.69))
    return (base[:, None] * jitter).reshape(HEADS * ATTENTION_SPAN).astype(jnp.float32)


def draw_additional_damping_exponent(key, part):
    rate_key, place_key, size_key = jax.random.split(jax.random.fold_in(key, 23), 3)
    rates = jnp.exp(jax.random.uniform(rate_key, (SEQS_ALL, 16, HEADS), jnp.float32, math.log(0.1), 0.0)) / LEN
    rates = jnp.repeat(rates, LEN // 16, axis=1)
    places = jax.random.randint(place_key, (SEQS_ALL, 3), 0, LEN)
    positions = jnp.arange(LEN, dtype=jnp.int32)
    hits = jnp.sum((positions[None, :, None] == places[:, None, :]).astype(jnp.float32), axis=2)
    strength = jax.random.uniform(size_key, (SEQS_ALL, 1, HEADS), jnp.float32, 0.22, 0.69)
    return (-rates - hits[:, :, None] * strength).astype(jnp.float32)


def block_levels(stream_key, shape, cuts, low, top_value):
    def one(dim, blocks):
        steps = jax.random.uniform(jax.random.fold_in(jax.random.fold_in(stream_key, 6), dim), (blocks,), jnp.float32, low / len(cuts), top_value / len(cuts))
        return jnp.repeat(jnp.exp(steps), shape[dim] // blocks).reshape((-1,) + (1,) * (len(shape) - dim - 1))

    level = one(*cuts[0])
    for cut in cuts[1:]:
        level = level * one(*cut)
    return level


def noise(own_key, shape, width, limit, pieces=(), held_as=jnp.bfloat16):
    result = jax.random.normal(own_key, shape, jnp.float32) * width
    if len(pieces) > 0:
        result = block_levels(own_key, shape, pieces, -0.22, 0.18) * result
    return jnp.clip(result, min=-limit, max=limit).astype(held_as)


def setup_inputs(seed: int = 0) -> dict:
    splits = jax.random.split(jax.random.key(seed), 10)
    return {
        "tokens": draw_tokens(jax.random.fold_in(splits[9], 71), 0),
        "first_token_input": noise(splits[1], (SEQS_ALL, D), 1.0, 6.0, ((0, 2), (1, 16))),
        "forget_weight": draw_forget_weight(jax.random.fold_in(splits[9], 71), 0),
        "value_weight": noise(splits[3], (D, HW), (D // 16) ** -0.5, 0.375, ((1, 8),)),
        "query_weight": noise(splits[4], (D, HW), D ** -0.5, 0.09375, ((0, 16), (1, 8))),
        "output_gate_weight": noise(splits[5], (D, HW), D ** -0.5, 0.09375, ((0, 16), (1, 8))),
        "forget_bound_slack": draw_forget_bound_slack(jax.random.fold_in(splits[9], 71), 0),
        "additional_damping_exponent": draw_additional_damping_exponent(jax.random.fold_in(splits[9], 71), 0),
        "read_norm_scale": jnp.clip(1.0 + 0.18 * jax.random.normal(splits[8], (ATTENTION_SPAN,), jnp.float32), 0.1, 1.9),
    }


def reference(tokens, first_token_input, forget_weight, value_weight, query_weight, output_gate_weight, forget_bound_slack, additional_damping_exponent, read_norm_scale):

    def sequence_wise(couple_bundle):
        series_lines, segment_damping_exponent = couple_bundle
        forget = jnp.dot(series_lines, forget_weight, preferred_element_type=jnp.float32).astype(jnp.bfloat16)
        values = jnp.dot(series_lines, value_weight, preferred_element_type=jnp.float32).astype(jnp.bfloat16)
        valve_sampler_seeds = forget_bound_slack * jax.nn.sigmoid(-forget.astype(jnp.float32))
        damping_exponent = jnp.log1p(-valve_sampler_seeds) + jnp.repeat(segment_damping_exponent, ATTENTION_SPAN, axis=1)
        later_sum = jnp.cumsum(damping_exponent[::-1], axis=0)[::-1] - damping_exponent
        weighted = (valve_sampler_seeds * jnp.exp(later_sum)).astype(jnp.bfloat16)
        key_weights = weighted.astype(jnp.float32).reshape(LEN, HEADS, ATTENTION_SPAN)
        value_rows = values.astype(jnp.float32).reshape(LEN, HEADS, ATTENTION_SPAN)
        return jnp.einsum('lha,lhb->hab', key_weights, value_rows).astype(jnp.bfloat16)
    cache = lax.map(sequence_wise, (tokens, additional_damping_exponent))
    new_query = jnp.dot(first_token_input, query_weight, preferred_element_type=jnp.float32).astype(jnp.bfloat16)
    new_gate = jnp.dot(first_token_input, output_gate_weight, preferred_element_type=jnp.float32).astype(jnp.bfloat16)
    new_forget = jnp.dot(first_token_input, forget_weight, preferred_element_type=jnp.float32).astype(jnp.bfloat16)
    new_value = jnp.dot(first_token_input, value_weight, preferred_element_type=jnp.float32).astype(jnp.bfloat16)
    seq_count = first_token_input.shape[0]
    new_keys = (forget_bound_slack * jax.nn.sigmoid(-new_forget.astype(jnp.float32))).reshape(seq_count, HEADS, ATTENTION_SPAN)
    value_new = new_value.astype(jnp.float32).reshape(seq_count, HEADS, ATTENTION_SPAN)
    updated = (1.0 - new_keys)[..., None] * cache.astype(jnp.float32) + new_keys[..., None] * value_new[:, :, None, :]
    query_rows = new_query.astype(jnp.float32).reshape(seq_count, HEADS, ATTENTION_SPAN)
    read_sum = jnp.einsum('sha,shab->shb', query_rows, updated, precision=lax.Precision.HIGHEST)
    scaled = read_sum * lax.rsqrt(lax.optimization_barrier(jnp.mean(read_sum * read_sum, axis=-1, keepdims=True)) + 1e-06) * read_norm_scale
    first_read = (scaled.reshape(seq_count, HEADS * ATTENTION_SPAN) * jax.nn.silu(new_gate.astype(jnp.float32))).astype(jnp.bfloat16)
    return (cache, first_read)
```

```python
import functools

import jax
import jax.numpy as jnp
from jax import lax
from jax.experimental import pallas as pl
from jax.experimental.pallas import tpu as pltpu
from jax.sharding import PartitionSpec as P


BF = jnp.bfloat16
F32 = jnp.float32


def three_terms(x):
    high = x.astype(BF)
    rest = x - high.astype(F32)
    middle = rest.astype(BF)
    low = (rest - middle.astype(F32)).astype(BF)
    return high, middle, low


def add_pieces(index_ref, step, pieces, wf_ref, wv_ref, f_in, v_in, f_out, v_out):
    for n, piece in enumerate(pieces):

        @pl.when(step == n)
        def _(piece=piece, n=n):
            x = piece[...]
            f = jnp.dot(x, wf_ref[...], preferred_element_type=F32)
            v = jnp.dot(x, wv_ref[...], preferred_element_type=F32)
            if n > 0:
                f_out[...] += f
                v_out[...] += v
            elif f_in is not None:
                f_out[...] = f_in[...] + f
                v_out[...] = v_in[...] + v
            else:
                f_out[...] = f
                v_out[...] = v


def project_kernel(index_ref, *refs, count, has_sums):
    pieces, refs = refs[:count], refs[count:]
    wf_ref, wv_ref, *refs = refs
    f_in, v_in = refs[:2] if has_sums else (None, None)
    f_out, v_out = refs[-2:]
    add_pieces(index_ref, pl.program_id(0), pieces, wf_ref, wv_ref, f_in, v_in, f_out, v_out)


def whole(shape):
    return pl.BlockSpec(shape, lambda i, index: (0,) * len(shape))


def weight_specs(width, channels):
    spec = pl.BlockSpec((width, channels), lambda i, index: (index[i], 0))
    return [spec, spec]


def project(index, pieces, weights, sums=()):
    rows, width = pieces[0].shape
    channels = weights[0].shape[1]
    out = jax.ShapeDtypeStruct((rows, channels), F32)
    return pl.pallas_call(
        functools.partial(project_kernel, count=len(pieces), has_sums=bool(sums)),
        grid_spec=pltpu.PrefetchScalarGridSpec(
            num_scalar_prefetch=1,
            grid=(len(pieces),),
            in_specs=[whole(p.shape) for p in pieces]
            + weight_specs(width, channels)
            + [whole(s.shape) for s in sums],
            out_specs=[whole((rows, channels))] * 2,
        ),
        out_shape=[out, out],
        name="project",
    )(index, *pieces, *weights, *sums)


def state_kernel(index_ref, *refs, count, seqs, heads, head_dim, parts):
    pieces, refs = refs[:count], refs[count:]
    wf_ref, wv_ref, f_in, v_in, slack_ref, damp_ref, out_ref, f_acc, v_acc = refs
    step = pl.program_id(0)
    add_pieces(index_ref, step, pieces, wf_ref, wv_ref, f_in, v_in, f_acc, v_acc)

    @pl.when(step == count - 1)
    def _():
        length = damp_ref.shape[1]
        row = lax.broadcasted_iota(jnp.int32, (length, length), 0)
        column = lax.broadcasted_iota(jnp.int32, (length, length), 1)
        later = jnp.where(column > row, 1.0, 0.0).astype(BF)
        ones = jnp.ones((length, head_dim), BF)
        lane = lax.broadcasted_iota(jnp.int32, (head_dim, head_dim), 1)
        totals = jnp.zeros((head_dim, head_dim), F32)
        pairs = seqs * heads
        over_rows = (((0,), (0,)), ((), ()))
        for s in range(seqs):
            for h in range(heads):
                rows, cols = pl.ds(s * length, length), pl.ds(h * head_dim, head_dim)
                forget = f_acc[rows, cols].astype(BF).astype(F32)
                values = v_acc[rows, cols].astype(BF)
                gate = slack_ref[:, cols] * jax.nn.sigmoid(-forget)
                decay = jnp.log1p(-gate) + damp_ref[s, :, h : h + 1]
                terms = three_terms(decay)
                within = sum(jnp.dot(later, t, preferred_element_type=F32) for t in terms)
                weighted = (gate * jnp.exp(within)).astype(BF)
                state = lax.dot_general(weighted, values, over_rows, preferred_element_type=F32)
                total = sum(
                    lax.dot_general(t, ones, over_rows, preferred_element_type=F32) for t in terms
                )
                totals = jnp.where(lane % 16 == s * heads + h, total, totals)
                out_ref[:, s * heads + h] = state.astype(BF).reshape(parts, head_dim // parts, head_dim)
        high, middle, low = three_terms(totals)
        packed = jnp.where(lane < 16, high, jnp.where(lane < 32, middle, low))
        packed = jnp.where(lane < 48, packed, jnp.zeros_like(packed))
        out_ref[:, pairs] = packed.reshape(parts, head_dim // parts, head_dim)


def states(index, pieces, weights, sums, slack, damp, parts):
    rows, width = pieces[0].shape
    channels = weights[0].shape[1]
    seqs, length, heads = damp.shape
    head_dim = channels // heads
    shape = (parts, seqs * heads + 1, head_dim // parts, head_dim)
    return pl.pallas_call(
        functools.partial(
            state_kernel, count=len(pieces), seqs=seqs, heads=heads, head_dim=head_dim, parts=parts
        ),
        grid_spec=pltpu.PrefetchScalarGridSpec(
            num_scalar_prefetch=1,
            grid=(len(pieces),),
            in_specs=[whole(p.shape) for p in pieces]
            + weight_specs(width, channels)
            + [whole(a.shape) for a in (*sums, slack, damp)],
            out_specs=whole(shape),
            scratch_shapes=[pltpu.VMEM((rows, channels), F32)] * 2,
        ),
        out_shape=jax.ShapeDtypeStruct(shape, BF),
        name="states",
    )(index, *pieces, *weights, *sums, slack, damp)


def combine_kernel(got_ref, query_ref, keys_ref, value_ref, cache_ref, read_ref):
    parts, pairs = got_ref.shape[0], got_ref.shape[1] - 1
    head_dim = got_ref.shape[3]
    rows = got_ref.shape[2]
    after = jnp.zeros((rows, head_dim), F32)
    sums = [jnp.zeros((rows, head_dim), F32)] * pairs
    for src in range(parts - 1, -1, -1):
        scale = jnp.exp(after)
        for j in range(pairs):
            sums[j] = sums[j] + scale[:, j : j + 1] * got_ref[src, j].astype(F32)
        packed = got_ref[src, pairs].astype(F32)
        after = after + (
            packed + pltpu.roll(packed, head_dim - 16, 1) + pltpu.roll(packed, head_dim - 32, 1)
        )
    for j in range(pairs):
        rounded = sums[j].astype(BF)
        cache_ref[j] = rounded
        keys = keys_ref[:, j : j + 1]
        updated = (1.0 - keys) * rounded.astype(F32) + keys * value_ref[j : j + 1, :]
        read_ref[j : j + 1, :] = jnp.sum(query_ref[:, j : j + 1] * updated, axis=0, keepdims=True)


def combine(got, query, keys, value):
    parts, tiles, rows, head_dim = got.shape
    pairs = tiles - 1
    return pl.pallas_call(
        combine_kernel,
        out_shape=[
            jax.ShapeDtypeStruct((pairs, rows, head_dim), BF),
            jax.ShapeDtypeStruct((pairs, head_dim), F32),
        ],
        name="combine",
    )(got, query, keys, value)


def finish_kernel(got_ref, norm_ref, gate_ref, out_ref):
    heads = out_ref.shape[1] // got_ref.shape[2]
    head_dim = got_ref.shape[2]
    read = got_ref[0]
    for src in range(1, got_ref.shape[0]):
        read = read + got_ref[src]
    scaled = read * lax.rsqrt(jnp.mean(read * read, axis=1, keepdims=True) + 1e-06) * norm_ref[...]
    result = (scaled * gate_ref[...]).astype(BF)
    for s in range(out_ref.shape[0]):
        for h in range(heads):
            j = s * heads + h
            out_ref[s : s + 1, h * head_dim : (h + 1) * head_dim] = result[j : j + 1, :]


def new_token_kernel(index_ref, x_ref, q_ref, g_ref, f_ref, v_ref, out_ref):
    x = x_ref[...]
    seqs = x.shape[0]
    for n, w in enumerate((q_ref, g_ref, f_ref, v_ref)):
        y = jnp.dot(x, w[...], preferred_element_type=F32)
        for p in range(out_ref.shape[0]):
            out_ref[p, n * seqs : (n + 1) * seqs, :] = y


def per_device(
    tokens,
    first_token_input,
    forget_weight,
    value_weight,
    query_weight,
    output_gate_weight,
    forget_bound_slack,
    additional_damping_exponent,
    read_norm_scale,
):
    seqs, length, width = tokens.shape
    head_dim = read_norm_scale.shape[0]
    heads = additional_damping_exponent.shape[2]
    channels = heads * head_dim
    sp_count = lax.axis_size("sp")
    sp = lax.axis_index("sp")
    tp_count = lax.axis_size("tp")
    tp = lax.axis_index("tp")
    chips = tp_count // 2
    chip, core = tp // 2, tp % 2
    weights = (forget_weight, value_weight)

    def shifted(x, by):
        return lax.ppermute(
            x, "tp", [(2 * c + k, 2 * ((c + by) % chips) + k) for c in range(chips) for k in (0, 1)]
        )

    def sibling(x):
        return lax.ppermute(x, "tp", [(i, i ^ 1) for i in range(tp_count)])

    def places(by):
        first = 2 * ((chip - by) % chips)
        return [first + core, first + 1 - core]

    def table(*entries):
        return jnp.stack(entries).astype(jnp.int32)

    half = seqs // 2
    rows = half * length
    own = tokens.reshape(seqs * length, width)
    own_a, own_b = own[:rows], own[rows:]
    others = sibling(own)
    right_a, left_a = shifted(own_a, 1), shifted(own_a, -1)
    right_b, left_b = shifted(own_b, 1), shifted(own_b, -1)

    slab = first_token_input.shape[1]
    partial = pl.pallas_call(
        new_token_kernel,
        grid_spec=pltpu.PrefetchScalarGridSpec(
            num_scalar_prefetch=1,
            grid=(1,),
            in_specs=[
                whole(first_token_input.shape),
                whole(query_weight.shape),
                whole(output_gate_weight.shape),
                pl.BlockSpec((slab, channels), lambda i, index: (index[0], 0)),
                pl.BlockSpec((slab, channels), lambda i, index: (index[0], 0)),
            ],
            out_specs=whole((sp_count, 4 * seqs, channels)),
        ),
        out_shape=jax.ShapeDtypeStruct((sp_count, 4 * seqs, channels), F32),
        name="new_token",
    )(table(sp), first_token_input, query_weight, output_gate_weight, *weights)
    new_sums = jnp.sum(lax.all_to_all(partial, "sp", 0, 0, tiled=True), axis=0).astype(BF).astype(F32)
    new_query, new_gate, new_forget, new_value = new_sums.reshape(4, seqs, channels)
    new_keys = forget_bound_slack * jax.nn.sigmoid(-new_forget)
    row_count = head_dim // sp_count

    def own_rows(x):
        x = lax.dynamic_slice_in_dim(
            x.reshape(seqs * heads, head_dim), sp * row_count, row_count, 1
        )
        return x.T

    query_rows, key_rows = own_rows(new_query), own_rows(new_keys)
    value_new = new_value.reshape(seqs * heads, head_dim)
    gate_new = jax.nn.silu(new_gate).reshape(seqs * heads, head_dim)

    sums = project(table(tp, tp + 1 - 2 * core), [own, others], weights)
    sums_a, sums_b = [s[:rows] for s in sums], [s[rows:] for s in sums]

    far_a = shifted(right_a, 1)
    other_near_a = sibling(jnp.concatenate([right_a, left_a]))
    far_b = shifted(left_b, -1)
    other_near_b = sibling(jnp.concatenate([right_b, left_b]))
    other_far_a = sibling(far_a)
    other_far_b = sibling(far_b)
    behind, ahead, across = places(1), places(-1), places(2)
    near_index = table(behind[0], ahead[0])
    other_near_index = table(behind[1], ahead[1])
    far_index = table(*across)
    slack = forget_bound_slack.reshape(1, channels)

    def near(sums, right, left, other_near):
        sums = project(near_index, [right, left], weights, sums)
        return project(other_near_index, [other_near[:rows], other_near[rows:]], weights, sums)

    def sent(sums, far, other_far, damp):
        out = states(far_index, [far, other_far], weights, sums, slack, damp, sp_count)
        return lax.all_to_all(out, "sp", 0, 0, tiled=True)

    sums_a = near(sums_a, right_a, left_a, other_near_a)
    sums_b = near(sums_b, right_b, left_b, other_near_b)
    got_a = sent(sums_a, far_a, other_far_a, additional_damping_exponent[:half])
    got_b = sent(sums_b, far_b, other_far_b, additional_damping_exponent[half:])

    pairs = half * heads
    cache_a, read_a = combine(got_a, query_rows[:, :pairs], key_rows[:, :pairs], value_new[:pairs])
    cache_b, read_b = combine(got_b, query_rows[:, pairs:], key_rows[:, pairs:], value_new[pairs:])
    read = jnp.concatenate([read_a, read_b])
    got = lax.all_to_all(
        jnp.broadcast_to(read[None], (sp_count, *read.shape)), "sp", 0, 0, tiled=True
    )
    first_read = pl.pallas_call(
        finish_kernel,
        out_shape=jax.ShapeDtypeStruct((seqs, channels), BF),
        name="finish",
    )(got, read_norm_scale.reshape(1, head_dim), gate_new)
    cache = jnp.concatenate([cache_a, cache_b]).reshape(seqs, heads, row_count, head_dim)
    return cache, first_read


def solution(mesh):
    placed = (
        P("gr", "sp", "tp"),
        P("gr", "sp"),
        P(None, "tp"),
        P(None, "tp"),
        P("sp", "tp"),
        P("sp", "tp"),
        P("tp"),
        P("gr", "sp", "tp"),
        P(),
    )
    return jax.shard_map(
        per_device,
        mesh=mesh,
        in_specs=placed,
        out_specs=(P("gr", "tp", "sp", None), P("gr", "tp")),
        check_vma=False,
    )
```

```python
import functools

import jax
import jax.numpy as jnp
from jax import lax
from jax.experimental import pallas as pl
from jax.experimental.pallas import tpu as pltpu
from jax.sharding import PartitionSpec as P


BF = jnp.bfloat16
F32 = jnp.float32


def three_terms(x):
    high = x.astype(BF)
    rest = x - high.astype(F32)
    middle = rest.astype(BF)
    low = (rest - middle.astype(F32)).astype(BF)
    return high, middle, low


VMEM = pl.BlockSpec(memory_space=pltpu.VMEM)


def in_vmem(kernel, out_shape, *arrays, in_specs=None, scratch=(), flops=0):
    return pl.pallas_call(
        kernel,
        in_specs=in_specs or [VMEM] * len(arrays),
        out_specs=jax.tree.map(lambda _: VMEM, out_shape),
        out_shape=out_shape,
        scratch_shapes=scratch,
        compiler_params=pltpu.CompilerParams(vmem_limit_bytes=12 << 20),
        cost_estimate=pl.CostEstimate(flops=flops, transcendentals=0, bytes_accessed=0),
    )(*arrays)


def copied(pairs, sems):
    copies = [pltpu.make_async_copy(*pair, sems.at[n]) for n, pair in enumerate(pairs)]
    for copy in copies:
        copy.start()
    for copy in copies:
        copy.wait()


def from_hbm(kernel, shapes, *arrays):
    return pl.pallas_call(
        kernel,
        in_specs=[pl.BlockSpec(memory_space=pltpu.HBM)] * len(arrays),
        out_specs=[VMEM] * len(shapes),
        out_shape=[pltpu.VMEM(shape, BF) for shape in shapes],
        scratch_shapes=[pltpu.SemaphoreType.DMA((len(shapes),))],
        compiler_params=pltpu.CompilerParams(vmem_limit_bytes=1 << 20),
    )(*(pltpu.with_memory_space_constraint(a, pltpu.HBM) for a in arrays))


def load_kernel(*refs):
    count = len(refs) // 2
    copied(list(zip(refs[:count], refs[count:-1])), refs[-1])


def load(*arrays):
    return from_hbm(load_kernel, [a.shape for a in arrays], *arrays)


def split_kernel(tokens_ref, *refs):
    seqs = tokens_ref.shape[0] // (len(refs) - 1)
    copied(
        [(tokens_ref.at[pl.ds(n * seqs, seqs)], out) for n, out in enumerate(refs[:-1])], refs[-1]
    )


def split(tokens, count):
    shape = (tokens.shape[0] // count, *tokens.shape[1:])
    return from_hbm(split_kernel, [shape] * count, tokens)


def block_of(tp, by, other):
    count = lax.axis_size("tp")
    return lax.rem((tp ^ 1 if other else tp) + count - 2 * by, count)


def products(pieces, sources, w_ref):
    tp = lax.axis_index("tp")
    total = None
    for piece, source in zip(pieces, sources):
        width = piece.shape[1]
        start = pl.multiple_of(block_of(tp, *source) * width, width)
        part = jnp.dot(piece[...], w_ref[pl.ds(start, width), :], preferred_element_type=F32)
        total = part if total is None else total + part
    return total


def project_kernel(*refs, sources, has_sums):
    count = len(sources)
    pieces, (wf_ref, wv_ref, *refs) = refs[:count], refs[count:]
    for n, w_ref in enumerate((wf_ref, wv_ref)):
        result = products(pieces, sources, w_ref)
        refs[-2 + n][...] = refs[n][...] + result if has_sums else result


def project(pieces, sources, weights, sums=()):
    rows, width = pieces[0].shape
    channels = weights[0].shape[1]
    return in_vmem(
        functools.partial(project_kernel, sources=sources, has_sums=bool(sums)),
        [jax.ShapeDtypeStruct((rows, channels), F32)] * 2,
        *pieces,
        *weights,
        *sums,
        flops=4 * len(pieces) * rows * width * channels,
    )


def state_kernel(*refs, sources, groups, head_dim):
    count = len(sources)
    pieces, refs = refs[: groups * count], refs[groups * count :]
    wf_ref, wv_ref, *refs = refs
    sums, (slack_ref, damp_ref, out_ref, f_acc, v_acc) = refs[: 2 * groups], refs[2 * groups :]
    rows = pieces[0].shape[0]
    for g in range(groups):
        here = pl.ds(g * rows, rows)
        group = pieces[g * count : (g + 1) * count]
        f_acc[here, :] = sums[2 * g][...] + products(group, sources, wf_ref)
        v_acc[here, :] = sums[2 * g + 1][...] + products(group, sources, wv_ref)
    parts = out_ref.shape[0]
    seqs, heads, length = damp_ref.shape
    channels = heads * head_dim
    row = lax.broadcasted_iota(jnp.int32, (length, length), 0)
    column = lax.broadcasted_iota(jnp.int32, (length, length), 1)
    later = jnp.where(column > row, 1.0, 0.0).astype(BF)
    head = lax.broadcasted_iota(jnp.int32, (heads, channels), 0)
    channel = lax.broadcasted_iota(jnp.int32, (heads, channels), 1)
    spread = jnp.where(channel // head_dim == head, 1.0, 0.0).astype(BF)
    over_rows = (((0,), (0,)), ((), ()))
    totals = []
    for s in range(seqs):
        here = pl.ds(s * length, length)
        forget = f_acc[here, :].astype(BF).astype(F32)
        values = v_acc[here, :].astype(BF)
        gate = slack_ref[...] * jax.nn.sigmoid(-forget)
        damping = sum(
            lax.dot_general(t, spread, over_rows, preferred_element_type=F32)
            for t in three_terms(damp_ref[s])
        )
        decay = jnp.log1p(-gate) + damping
        within = sum(jnp.dot(later, t, preferred_element_type=F32) for t in three_terms(decay))
        weighted = (gate * jnp.exp(within)).astype(BF)
        total = within[:1, :] + decay[:1, :]
        for h in range(heads):
            cols = slice(h * head_dim, (h + 1) * head_dim)
            state = lax.dot_general(
                weighted[:, cols], values[:, cols], over_rows, preferred_element_type=F32
            )
            totals.append(total[:, cols])
            out_ref[:, s * heads + h] = state.astype(BF).reshape(parts, head_dim // parts, head_dim)
    pairs = seqs * heads
    terms = [t.astype(F32) for t in three_terms(jnp.concatenate(totals))]
    packed = jnp.concatenate([*terms, jnp.zeros((head_dim - 3 * pairs, head_dim), F32)])
    out_ref[:, pairs] = packed.T.astype(BF).reshape(parts, head_dim // parts, head_dim)


def states(pieces, sources, weights, sums, slack, damp, parts):
    rows, width = pieces[0].shape
    channels = weights[0].shape[1]
    seqs, heads, _ = damp.shape
    head_dim = channels // heads
    groups = len(pieces) // len(sources)
    return in_vmem(
        functools.partial(state_kernel, sources=sources, groups=groups, head_dim=head_dim),
        jax.ShapeDtypeStruct((parts, seqs * heads + 1, head_dim // parts, head_dim), BF),
        *pieces,
        *weights,
        *sums,
        slack,
        damp,
        scratch=[pltpu.VMEM((groups * rows, channels), F32)] * 2,
        flops=12 * len(pieces) * rows * width * channels,
    )


def combine_kernel(got_ref, query_ref, keys_ref, value_ref, cache_ref, read_ref):
    parts, pairs = got_ref.shape[0], got_ref.shape[1] - 1
    rows, head_dim = got_ref.shape[2:]
    after = jnp.zeros((rows, head_dim), F32)
    sums = [jnp.zeros((rows, head_dim), F32)] * pairs
    for src in range(parts - 1, -1, -1):
        scale = jnp.exp(after)
        for j in range(pairs):
            sums[j] = sums[j] + scale[:, j : j + 1] * got_ref[src, j].astype(F32)
        packed = got_ref[src, pairs].astype(F32)
        after = after + (
            packed
            + pltpu.roll(packed, head_dim - pairs, 1)
            + pltpu.roll(packed, head_dim - 2 * pairs, 1)
        )
    reads = []
    for j in range(pairs):
        rounded = sums[j].astype(BF)
        cache_ref[j] = rounded
        keys = keys_ref[:, j : j + 1]
        updated = (1.0 - keys) * rounded.astype(F32) + keys * value_ref[j : j + 1, :]
        reads.append(jnp.sum(query_ref[:, j : j + 1] * updated, axis=0, keepdims=True))
    reads = jnp.concatenate(reads)
    for p in range(parts):
        read_ref[p] = reads


def combine(got, query, keys, value):
    parts, tiles, rows, head_dim = got.shape
    return in_vmem(
        combine_kernel,
        [
            jax.ShapeDtypeStruct((tiles - 1, rows, head_dim), BF),
            jax.ShapeDtypeStruct((parts, tiles - 1, head_dim), F32),
        ],
        got,
        query,
        keys,
        value,
    )


def finish_kernel(got_ref, norm_ref, gate_ref, out_ref):
    heads = out_ref.shape[1] // got_ref.shape[2]
    head_dim = got_ref.shape[2]
    read = got_ref[0]
    for src in range(1, got_ref.shape[0]):
        read = read + got_ref[src]
    scaled = read * lax.rsqrt(jnp.mean(read * read, axis=1, keepdims=True) + 1e-06) * norm_ref[...]
    result = (scaled * gate_ref[...]).astype(BF)
    for s in range(out_ref.shape[0]):
        for h in range(heads):
            j = s * heads + h
            out_ref[s : s + 1, h * head_dim : (h + 1) * head_dim] = result[j : j + 1, :]


def new_token_kernel(x_ref, q_ref, g_ref, f_hbm, v_hbm, out_ref, f_rows, v_rows, sems):
    x = x_ref[...]
    seqs, slab = x.shape
    here = pl.ds(pl.multiple_of(lax.axis_index("sp") * slab, slab), slab)
    copied([(f_hbm.at[here], f_rows), (v_hbm.at[here], v_rows)], sems)
    for n, w in enumerate((q_ref, g_ref, f_rows, v_rows)):
        y = jnp.dot(x, w[...], preferred_element_type=F32)
        for p in range(out_ref.shape[0]):
            out_ref[p, n * seqs : (n + 1) * seqs, :] = y


def prepare_kernel(got_ref, slack_ref, query_ref, keys_ref, value_ref, gate_ref):
    pairs, head_dim = value_ref.shape
    rows = query_ref.shape[0]
    seqs = got_ref.shape[1] // 4
    heads = pairs // seqs
    total = got_ref[0]
    for src in range(1, got_ref.shape[0]):
        total = total + got_ref[src]
    rounded = total.astype(BF).astype(F32)

    def by_head(x):
        return jnp.concatenate(
            [
                x[s : s + 1, h * head_dim : (h + 1) * head_dim]
                for s in range(x.shape[0])
                for h in range(heads)
            ]
        )

    query, gate, forget, value = (rounded[n * seqs : (n + 1) * seqs] for n in range(4))
    keys = slack_ref[...] * jax.nn.sigmoid(-forget)
    value_ref[...] = by_head(value)
    gate_ref[...] = by_head(gate * jax.nn.sigmoid(gate))
    own = lax.axis_index("sp") * rows + lax.broadcasted_iota(jnp.int32, (rows, head_dim), 0)
    chosen = jnp.where(lax.broadcasted_iota(jnp.int32, (rows, head_dim), 1) == own, 1.0, 0.0).astype(BF)

    def own_rows(x):
        return sum(
            lax.dot_general(chosen, t, (((1,), (1,)), ((), ())), preferred_element_type=F32)
            for t in three_terms(x)
        )

    query_ref[...] = own_rows(by_head(query))
    keys_ref[...] = own_rows(by_head(keys))


def per_device(
    tokens,
    first_token_input,
    forget_weight,
    value_weight,
    query_weight,
    output_gate_weight,
    forget_bound_slack,
    additional_damping_exponent,
    read_norm_scale,
):
    seqs, length, width = tokens.shape
    head_dim = read_norm_scale.shape[0]
    heads = additional_damping_exponent.shape[2]
    channels = heads * head_dim
    sp_count = lax.axis_size("sp")
    tp_count = lax.axis_size("tp")
    chips = tp_count // 2
    slack = forget_bound_slack.reshape(1, channels)

    def shifted(x, by):
        pairs = [(2 * c + k, 2 * ((c + by) % chips) + k) for c in range(chips) for k in (0, 1)]
        return lax.ppermute(x, "tp", pairs)

    def sibling(x):
        return lax.ppermute(x, "tp", [(i, i ^ 1) for i in range(tp_count)])

    def exchange(x):
        return lax.all_to_all(x, "sp", 0, 0, tiled=True)

    rows = seqs // 2 * length
    own_a, own_b = (x.reshape(rows, width) for x in split(tokens, 2))
    right_a, left_a = shifted(own_a, 1), shifted(own_a, -1)
    right_b, left_b = shifted(own_b, 1), shifted(own_b, -1)
    other_a, other_b = sibling(own_a), sibling(own_b)

    partial = in_vmem(
        new_token_kernel,
        jax.ShapeDtypeStruct((sp_count, 4 * seqs, channels), F32),
        first_token_input,
        query_weight,
        output_gate_weight,
        pltpu.with_memory_space_constraint(forget_weight, pltpu.HBM),
        pltpu.with_memory_space_constraint(value_weight, pltpu.HBM),
        in_specs=[VMEM] * 3 + [pl.BlockSpec(memory_space=pltpu.HBM)] * 2,
        scratch=[pltpu.VMEM(query_weight.shape, BF)] * 2 + [pltpu.SemaphoreType.DMA((2,))],
    )
    new_sums = exchange(partial)
    row_count = head_dim // sp_count
    pairs = seqs * heads
    query_rows, key_rows, value_new, gate_new = in_vmem(
        prepare_kernel,
        [jax.ShapeDtypeStruct((row_count, pairs), F32)] * 2
        + [jax.ShapeDtypeStruct((pairs, head_dim), F32)] * 2,
        new_sums,
        slack,
    )

    weights = load(forget_weight, value_weight)
    weights = [pltpu.with_memory_space_constraint(w, pltpu.VMEM) for w in weights]

    def projected(pieces, sources, sums=()):
        return project(pieces, sources, weights, sums)

    far_a = shifted(right_a, 1)
    other_right_a, other_left_a = sibling(right_a), sibling(left_a)
    far_b = shifted(left_b, -1)
    other_right_b, other_left_b = sibling(right_b), sibling(left_b)
    other_far_a, other_far_b = sibling(far_a), sibling(far_b)

    here = ((0, False), (0, True))
    near = ((1, False), (-1, False))
    other_near = ((1, True), (-1, True))
    sums_a = projected([own_a, other_a], here)
    sums_b = projected([own_b, other_b], here)
    sums_a = projected([right_a, left_a], near, sums_a)
    sums_a = projected([other_right_a, other_left_a], other_near, sums_a)
    sums_b = projected([right_b, left_b], near, sums_b)
    sums_b = projected([other_right_b, other_left_b], other_near, sums_b)

    out = states(
        [far_a, other_far_a, far_b, other_far_b],
        ((2, False), (2, True)),
        weights,
        [*sums_a, *sums_b],
        slack,
        additional_damping_exponent.transpose(0, 2, 1),
        sp_count,
    )
    got = exchange(out)
    cache, read = combine(got, query_rows, key_rows, value_new)
    got = exchange(read)
    first_read = in_vmem(
        finish_kernel,
        jax.ShapeDtypeStruct((seqs, channels), BF),
        got,
        read_norm_scale.reshape(1, head_dim),
        gate_new,
    )
    return cache.reshape(seqs, heads, row_count, head_dim), first_read


def solution(mesh):
    placed = (
        P("gr", "sp", "tp"),
        P("gr", "sp"),
        P(None, "tp"),
        P(None, "tp"),
        P("sp", "tp"),
        P("sp", "tp"),
        P("tp"),
        P("gr", "sp", "tp"),
        P(),
    )

    return jax.shard_map(
        per_device,
        mesh=mesh,
        in_specs=placed,
        out_specs=(P("gr", "tp", "sp", None), P("gr", "tp")),
        check_vma=False,
    )
```

```python
import functools

import jax
import jax.numpy as jnp
from jax import lax
from jax.experimental import pallas as pl
from jax.experimental.pallas import tpu as pltpu
from jax.sharding import PartitionSpec as P


BF = jnp.bfloat16
F32 = jnp.float32


def three_terms(x):
    high = x.astype(BF)
    rest = x - high.astype(F32)
    middle = rest.astype(BF)
    low = (rest - middle.astype(F32)).astype(BF)
    return high, middle, low


VMEM = pl.BlockSpec(memory_space=pltpu.VMEM)


def in_vmem(kernel, out_shape, *arrays, in_specs=None, scratch=(), flops=0):
    return pl.pallas_call(
        kernel,
        in_specs=in_specs or [VMEM] * len(arrays),
        out_specs=jax.tree.map(lambda _: VMEM, out_shape),
        out_shape=out_shape,
        scratch_shapes=scratch,
        compiler_params=pltpu.CompilerParams(vmem_limit_bytes=12 << 20),
        cost_estimate=pl.CostEstimate(flops=flops, transcendentals=0, bytes_accessed=0),
    )(*arrays)


def copied(pairs, sems):
    copies = [pltpu.make_async_copy(*pair, sems.at[n]) for n, pair in enumerate(pairs)]
    for copy in copies:
        copy.start()
    for copy in copies:
        copy.wait()


def from_hbm(kernel, shapes, *arrays):
    return pl.pallas_call(
        kernel,
        in_specs=[pl.BlockSpec(memory_space=pltpu.HBM)] * len(arrays),
        out_specs=[VMEM] * len(shapes),
        out_shape=[pltpu.VMEM(shape, BF) for shape in shapes],
        scratch_shapes=[pltpu.SemaphoreType.DMA((len(shapes),))],
        compiler_params=pltpu.CompilerParams(vmem_limit_bytes=1 << 20),
    )(*(pltpu.with_memory_space_constraint(a, pltpu.HBM) for a in arrays))


def load_kernel(*refs):
    count = len(refs) // 2
    copied(list(zip(refs[:count], refs[count:-1])), refs[-1])


def load(*arrays):
    return from_hbm(load_kernel, [a.shape for a in arrays], *arrays)


def split_kernel(tokens_ref, *refs):
    seqs = tokens_ref.shape[0] // (len(refs) - 1)
    copied(
        [(tokens_ref.at[pl.ds(n * seqs, seqs)], out) for n, out in enumerate(refs[:-1])], refs[-1]
    )


def split(tokens, count):
    shape = (tokens.shape[0] // count, *tokens.shape[1:])
    return from_hbm(split_kernel, [shape] * count, tokens)


def block_of(tp, by, other):
    count = lax.axis_size("tp")
    return lax.rem((tp ^ 1 if other else tp) + count - 2 * by, count)


def products(pieces, sources, w_ref):
    tp = lax.axis_index("tp")
    total = None
    for piece, source in zip(pieces, sources):
        width = piece.shape[1]
        start = pl.multiple_of(block_of(tp, *source) * width, width)
        part = jnp.dot(piece[...], w_ref[pl.ds(start, width), :], preferred_element_type=F32)
        total = part if total is None else total + part
    return total


def project_kernel(*refs, sources, has_sums):
    count = len(sources)
    pieces, (wf_ref, wv_ref, *refs) = refs[:count], refs[count:]
    for n, w_ref in enumerate((wf_ref, wv_ref)):
        result = products(pieces, sources, w_ref)
        refs[-2 + n][...] = refs[n][...] + result if has_sums else result


def project(pieces, sources, weights, sums=()):
    rows, width = pieces[0].shape
    channels = weights[0].shape[1]
    return in_vmem(
        functools.partial(project_kernel, sources=sources, has_sums=bool(sums)),
        [jax.ShapeDtypeStruct((rows, channels), F32)] * 2,
        *pieces,
        *weights,
        *sums,
        flops=4 * len(pieces) * rows * width * channels,
    )


def state_kernel(*refs, sources, groups, head_dim):
    count = len(sources)
    pieces, refs = refs[: groups * count], refs[groups * count :]
    wf_ref, wv_ref, *refs = refs
    sums, (slack_ref, damp_ref, out_ref, f_acc, v_acc) = refs[: 2 * groups], refs[2 * groups :]
    rows = pieces[0].shape[0]
    for g in range(groups):
        here = pl.ds(g * rows, rows)
        group = pieces[g * count : (g + 1) * count]
        f_acc[here, :] = sums[2 * g][...] + products(group, sources, wf_ref)
        v_acc[here, :] = sums[2 * g + 1][...] + products(group, sources, wv_ref)
    parts = out_ref.shape[0]
    seqs, heads, length = damp_ref.shape
    channels = heads * head_dim
    row = lax.broadcasted_iota(jnp.int32, (length, length), 0)
    column = lax.broadcasted_iota(jnp.int32, (length, length), 1)
    later = jnp.where(column > row, 1.0, 0.0).astype(BF)
    head = lax.broadcasted_iota(jnp.int32, (heads, channels), 0)
    channel = lax.broadcasted_iota(jnp.int32, (heads, channels), 1)
    spread = jnp.where(channel // head_dim == head, 1.0, 0.0).astype(BF)
    over_rows = (((0,), (0,)), ((), ()))
    totals = []
    for s in range(seqs):
        here = pl.ds(s * length, length)
        forget = f_acc[here, :].astype(BF).astype(F32)
        values = v_acc[here, :].astype(BF)
        gate = slack_ref[...] * jax.nn.sigmoid(-forget)
        damping = sum(
            lax.dot_general(t, spread, over_rows, preferred_element_type=F32)
            for t in three_terms(damp_ref[s])
        )
        decay = jnp.log1p(-gate) + damping
        within = sum(jnp.dot(later, t, preferred_element_type=F32) for t in three_terms(decay))
        weighted = (gate * jnp.exp(within)).astype(BF)
        total = within[:1, :] + decay[:1, :]
        for h in range(heads):
            cols = slice(h * head_dim, (h + 1) * head_dim)
            state = lax.dot_general(
                weighted[:, cols], values[:, cols], over_rows, preferred_element_type=F32
            )
            totals.append(total[:, cols])
            out_ref[:, s * heads + h] = state.astype(BF).reshape(parts, head_dim // parts, head_dim)
    pairs = seqs * heads
    terms = [t.astype(F32) for t in three_terms(jnp.concatenate(totals))]
    packed = jnp.concatenate([*terms, jnp.zeros((head_dim - 3 * pairs, head_dim), F32)])
    out_ref[:, pairs] = packed.T.astype(BF).reshape(parts, head_dim // parts, head_dim)


def states(pieces, sources, weights, sums, slack, damp, parts):
    rows, width = pieces[0].shape
    channels = weights[0].shape[1]
    seqs, heads, _ = damp.shape
    head_dim = channels // heads
    groups = len(pieces) // len(sources)
    return in_vmem(
        functools.partial(state_kernel, sources=sources, groups=groups, head_dim=head_dim),
        jax.ShapeDtypeStruct((parts, seqs * heads + 1, head_dim // parts, head_dim), BF),
        *pieces,
        *weights,
        *sums,
        slack,
        damp,
        scratch=[pltpu.VMEM((groups * rows, channels), F32)] * 2,
        flops=12 * len(pieces) * rows * width * channels,
    )


def combine_kernel(got_ref, query_ref, keys_ref, value_ref, cache_ref, read_ref):
    parts, pairs = got_ref.shape[0], got_ref.shape[1] - 1
    rows, head_dim = got_ref.shape[2:]
    after = jnp.zeros((rows, head_dim), F32)
    sums = [jnp.zeros((rows, head_dim), F32)] * pairs
    for src in range(parts - 1, -1, -1):
        scale = jnp.exp(after)
        for j in range(pairs):
            sums[j] = sums[j] + scale[:, j : j + 1] * got_ref[src, j].astype(F32)
        packed = got_ref[src, pairs].astype(F32)
        after = after + (
            packed
            + pltpu.roll(packed, head_dim - pairs, 1)
            + pltpu.roll(packed, head_dim - 2 * pairs, 1)
        )
    reads = []
    for j in range(pairs):
        rounded = sums[j].astype(BF)
        cache_ref[j] = rounded
        keys = keys_ref[:, j : j + 1]
        updated = (1.0 - keys) * rounded.astype(F32) + keys * value_ref[j : j + 1, :]
        reads.append(jnp.sum(query_ref[:, j : j + 1] * updated, axis=0, keepdims=True))
    reads = jnp.concatenate(reads)
    for p in range(parts):
        read_ref[p] = reads


def combine(got, query, keys, value):
    parts, tiles, rows, head_dim = got.shape
    return in_vmem(
        combine_kernel,
        [
            jax.ShapeDtypeStruct((tiles - 1, rows, head_dim), BF),
            jax.ShapeDtypeStruct((parts, tiles - 1, head_dim), F32),
        ],
        got,
        query,
        keys,
        value,
    )


def finish_kernel(got_ref, norm_ref, gate_ref, out_ref):
    heads = out_ref.shape[1] // got_ref.shape[2]
    head_dim = got_ref.shape[2]
    read = got_ref[0]
    for src in range(1, got_ref.shape[0]):
        read = read + got_ref[src]
    scaled = read * lax.rsqrt(jnp.mean(read * read, axis=1, keepdims=True) + 1e-06) * norm_ref[...]
    result = (scaled * gate_ref[...]).astype(BF)
    for s in range(out_ref.shape[0]):
        for h in range(heads):
            j = s * heads + h
            out_ref[s : s + 1, h * head_dim : (h + 1) * head_dim] = result[j : j + 1, :]


def new_token_kernel(x_ref, q_hbm, g_hbm, f_hbm, v_hbm, out_ref, x_here, rows, sems):
    seqs, slab = x_ref.shape
    here = pl.ds(pl.multiple_of(lax.axis_index("sp") * slab, slab), slab)
    sources = (q_hbm, g_hbm, f_hbm.at[here], v_hbm.at[here])
    copied([(w, rows.at[n]) for n, w in enumerate(sources)] + [(x_ref, x_here)], sems)
    for n in range(len(sources)):
        y = jnp.dot(x_here[...], rows[n], preferred_element_type=F32)
        for p in range(out_ref.shape[0]):
            out_ref[p, n * seqs : (n + 1) * seqs, :] = y


def prepare_kernel(got_ref, slack_ref, query_ref, keys_ref, value_ref, gate_ref):
    pairs, head_dim = value_ref.shape
    rows = query_ref.shape[0]
    seqs = got_ref.shape[1] // 4
    heads = pairs // seqs
    total = got_ref[0]
    for src in range(1, got_ref.shape[0]):
        total = total + got_ref[src]
    rounded = total.astype(BF).astype(F32)

    def by_head(x):
        return jnp.concatenate(
            [
                x[s : s + 1, h * head_dim : (h + 1) * head_dim]
                for s in range(x.shape[0])
                for h in range(heads)
            ]
        )

    query, gate, forget, value = (rounded[n * seqs : (n + 1) * seqs] for n in range(4))
    keys = slack_ref[...] * jax.nn.sigmoid(-forget)
    value_ref[...] = by_head(value)
    gate_ref[...] = by_head(gate * jax.nn.sigmoid(gate))
    own = lax.axis_index("sp") * rows + lax.broadcasted_iota(jnp.int32, (rows, head_dim), 0)
    chosen = jnp.where(lax.broadcasted_iota(jnp.int32, (rows, head_dim), 1) == own, 1.0, 0.0).astype(BF)

    def own_rows(x):
        return sum(
            lax.dot_general(chosen, t, (((1,), (1,)), ((), ())), preferred_element_type=F32)
            for t in three_terms(x)
        )

    query_ref[...] = own_rows(by_head(query))
    keys_ref[...] = own_rows(by_head(keys))


def per_device(
    tokens,
    first_token_input,
    forget_weight,
    value_weight,
    query_weight,
    output_gate_weight,
    forget_bound_slack,
    additional_damping_exponent,
    read_norm_scale,
):
    seqs, length, width = tokens.shape
    head_dim = read_norm_scale.shape[0]
    heads = additional_damping_exponent.shape[2]
    channels = heads * head_dim
    sp_count = lax.axis_size("sp")
    tp_count = lax.axis_size("tp")
    chips = tp_count // 2
    slack = forget_bound_slack.reshape(1, channels)

    def shifted(x, by):
        pairs = [(2 * c + k, 2 * ((c + by) % chips) + k) for c in range(chips) for k in (0, 1)]
        return lax.ppermute(x, "tp", pairs)

    def sibling(x):
        return lax.ppermute(x, "tp", [(i, i ^ 1) for i in range(tp_count)])

    def exchange(x):
        return lax.all_to_all(x, "sp", 0, 0, tiled=True)

    rows = seqs // 2 * length
    own_a, own_b = (x.reshape(rows, width) for x in split(tokens, 2))
    right_a, left_a = shifted(own_a, 1), shifted(own_a, -1)
    right_b, left_b = shifted(own_b, 1), shifted(own_b, -1)
    other_a, other_b = sibling(own_a), sibling(own_b)

    partial = in_vmem(
        new_token_kernel,
        jax.ShapeDtypeStruct((sp_count, 4 * seqs, channels), F32),
        *(
            pltpu.with_memory_space_constraint(x, pltpu.HBM)
            for x in (
                first_token_input,
                query_weight,
                output_gate_weight,
                forget_weight,
                value_weight,
            )
        ),
        in_specs=[pl.BlockSpec(memory_space=pltpu.HBM)] * 5,
        scratch=[
            pltpu.VMEM(first_token_input.shape, BF),
            pltpu.VMEM((4, *query_weight.shape), BF),
            pltpu.SemaphoreType.DMA((5,)),
        ],
    )
    new_sums = exchange(partial)
    row_count = head_dim // sp_count
    pairs = seqs * heads
    query_rows, key_rows, value_new, gate_new = in_vmem(
        prepare_kernel,
        [jax.ShapeDtypeStruct((row_count, pairs), F32)] * 2
        + [jax.ShapeDtypeStruct((pairs, head_dim), F32)] * 2,
        new_sums,
        slack,
    )

    weights = load(forget_weight, value_weight)
    weights = [pltpu.with_memory_space_constraint(w, pltpu.VMEM) for w in weights]

    def projected(pieces, sources, sums=()):
        return project(pieces, sources, weights, sums)

    far_a = shifted(right_a, 1)
    other_right_a, other_left_a = sibling(right_a), sibling(left_a)
    far_b = shifted(left_b, -1)
    other_right_b, other_left_b = sibling(right_b), sibling(left_b)
    other_far_a, other_far_b = sibling(far_a), sibling(far_b)

    here = ((0, False), (0, True))
    near = ((1, False), (-1, False))
    other_near = ((1, True), (-1, True))
    sums_a = projected([own_a, other_a], here)
    sums_b = projected([own_b, other_b], here)
    sums_a = projected([right_a, left_a], near, sums_a)
    sums_a = projected([other_right_a, other_left_a], other_near, sums_a)
    sums_b = projected([right_b, left_b], near, sums_b)
    sums_b = projected([other_right_b, other_left_b], other_near, sums_b)

    out = states(
        [far_a, other_far_a, far_b, other_far_b],
        ((2, False), (2, True)),
        weights,
        [*sums_a, *sums_b],
        slack,
        additional_damping_exponent.transpose(0, 2, 1),
        sp_count,
    )
    got = exchange(out)
    cache, read = combine(got, query_rows, key_rows, value_new)
    got = exchange(read)
    first_read = in_vmem(
        finish_kernel,
        jax.ShapeDtypeStruct((seqs, channels), BF),
        got,
        read_norm_scale.reshape(1, head_dim),
        gate_new,
    )
    return cache.reshape(seqs, heads, row_count, head_dim), first_read


def solution(mesh):
    placed = (
        P("gr", "sp", "tp"),
        P("gr", "sp"),
        P(None, "tp"),
        P(None, "tp"),
        P("sp", "tp"),
        P("sp", "tp"),
        P("tp"),
        P("gr", "sp", "tp"),
        P(),
    )

    return jax.shard_map(
        per_device,
        mesh=mesh,
        in_specs=placed,
        out_specs=(P("gr", "tp", "sp", None), P("gr", "tp")),
        check_vma=False,
    )
```

```python
import functools

import jax
import jax.numpy as jnp
from jax import lax
from jax.experimental import pallas as pl
from jax.experimental.pallas import tpu as pltpu
from jax.sharding import PartitionSpec as P


BF = jnp.bfloat16
F32 = jnp.float32


def three_terms(x):
    high = x.astype(BF)
    rest = x - high.astype(F32)
    middle = rest.astype(BF)
    low = (rest - middle.astype(F32)).astype(BF)
    return high, middle, low


VMEM = pl.BlockSpec(memory_space=pltpu.VMEM)


def in_vmem(kernel, out_shape, *arrays, in_specs=None, scratch=(), flops=0):
    return pl.pallas_call(
        kernel,
        in_specs=in_specs or [VMEM] * len(arrays),
        out_specs=jax.tree.map(lambda _: VMEM, out_shape),
        out_shape=out_shape,
        scratch_shapes=scratch,
        compiler_params=pltpu.CompilerParams(vmem_limit_bytes=12 << 20),
        cost_estimate=pl.CostEstimate(flops=flops, transcendentals=0, bytes_accessed=0),
    )(*arrays)


def copied(pairs, sems):
    copies = [pltpu.make_async_copy(*pair, sems.at[n]) for n, pair in enumerate(pairs)]
    for copy in copies:
        copy.start()
    for copy in copies:
        copy.wait()


def from_hbm(kernel, shapes, *arrays):
    return pl.pallas_call(
        kernel,
        in_specs=[pl.BlockSpec(memory_space=pltpu.HBM)] * len(arrays),
        out_specs=[VMEM] * len(shapes),
        out_shape=[pltpu.VMEM(shape, BF) for shape in shapes],
        scratch_shapes=[pltpu.SemaphoreType.DMA((len(shapes),))],
        compiler_params=pltpu.CompilerParams(vmem_limit_bytes=1 << 20),
    )(*(pltpu.with_memory_space_constraint(a, pltpu.HBM) for a in arrays))


def split_kernel(tokens_ref, *refs):
    seqs = tokens_ref.shape[0] // (len(refs) - 1)
    copied(
        [(tokens_ref.at[pl.ds(n * seqs, seqs)], out) for n, out in enumerate(refs[:-1])], refs[-1]
    )


def split(tokens, count):
    shape = (tokens.shape[0] // count, *tokens.shape[1:])
    return from_hbm(split_kernel, [shape] * count, tokens)


def block_of(tp, by, other):
    count = lax.axis_size("tp")
    return lax.rem((tp ^ 1 if other else tp) + count - 2 * by, count)


def products(pieces, sources, w_ref):
    tp = lax.axis_index("tp")
    total = None
    for piece, source in zip(pieces, sources):
        width = piece.shape[1]
        start = pl.multiple_of(block_of(tp, *source) * width, width)
        part = jnp.dot(piece[...], w_ref[pl.ds(start, width), :], preferred_element_type=F32)
        total = part if total is None else total + part
    return total


def add_products(pieces, plan, weights, sums, outs):
    rows = pieces[0].shape[0]
    for half, sources in enumerate(plan):
        here = pl.ds(half * rows, rows)
        some, pieces = pieces[: len(sources)], pieces[len(sources) :]
        for n, (w_ref, out) in enumerate(zip(weights, outs)):
            result = products(some, sources, w_ref)
            out[here, :] = sums[n][here, :] + result if sums else result


def project_kernel(*refs, plan):
    count = sum(map(len, plan))
    add_products(refs[:count], plan, refs[count : count + 2], refs[-4:-2], refs[-2:])


def project(pieces, plan, weights, sums):
    return in_vmem(
        functools.partial(project_kernel, plan=plan),
        [jax.ShapeDtypeStruct(s.shape, F32) for s in sums],
        *pieces,
        *weights,
        *sums,
        flops=4 * len(pieces) * pieces[0].size * weights[0].shape[1],
    )


def load_kernel(*refs, plan):
    count = sum(map(len, plan))
    pieces, (wf_hbm, wv_hbm, wf_ref, wv_ref, *outs, sems) = refs[:count], refs[count:]
    chips = lax.axis_size("tp") // 2
    depth = wf_ref.shape[0] // chips
    chip = lax.axis_index("tp") // 2
    copies = []
    for step in range(chips):
        here = pl.ds(pl.multiple_of(lax.rem(chip + step, chips) * depth, depth), depth)
        for n, (source, target) in enumerate(((wf_hbm, wf_ref), (wv_hbm, wv_ref))):
            copies.append(
                pltpu.make_async_copy(source.at[here], target.at[here], sems.at[2 * step + n])
            )
    for copy in copies:
        copy.start()
    for copy in copies[:2]:
        copy.wait()
    add_products(pieces, plan, (wf_ref, wv_ref), (), outs)
    for copy in copies[2:]:
        copy.wait()


def load_and_project(pieces, plan, weights):
    rows = len(plan) * pieces[0].shape[0]
    out = jax.ShapeDtypeStruct((rows, weights[0].shape[1]), F32)
    *weights, f, v = pl.pallas_call(
        functools.partial(load_kernel, plan=plan),
        in_specs=[VMEM] * len(pieces) + [pl.BlockSpec(memory_space=pltpu.HBM)] * 2,
        out_specs=[VMEM] * 4,
        out_shape=[pltpu.VMEM(w.shape, BF) for w in weights] + [out] * 2,
        scratch_shapes=[pltpu.SemaphoreType.DMA((lax.axis_size("tp"),))],
        compiler_params=pltpu.CompilerParams(vmem_limit_bytes=12 << 20),
        name="load",
    )(*pieces, *(pltpu.with_memory_space_constraint(w, pltpu.HBM) for w in weights))
    return [pltpu.with_memory_space_constraint(w, pltpu.VMEM) for w in weights], [f, v]


def state_kernel(*refs, plan, head_dim):
    count = sum(map(len, plan))
    pieces, (wf_ref, wv_ref, f_in, v_in, *refs) = refs[:count], refs[count:]
    slack_ref, damp_ref, out_ref, f_acc, v_acc = refs
    add_products(pieces, plan, (wf_ref, wv_ref), (f_in, v_in), (f_acc, v_acc))
    parts = out_ref.shape[0]
    seqs, heads, length = damp_ref.shape
    channels = heads * head_dim
    row = lax.broadcasted_iota(jnp.int32, (length, length), 0)
    column = lax.broadcasted_iota(jnp.int32, (length, length), 1)
    later = jnp.where(column > row, 1.0, 0.0).astype(BF)
    head = lax.broadcasted_iota(jnp.int32, (heads, channels), 0)
    channel = lax.broadcasted_iota(jnp.int32, (heads, channels), 1)
    spread = jnp.where(channel // head_dim == head, 1.0, 0.0).astype(BF)
    over_rows = (((0,), (0,)), ((), ()))
    totals = []
    for s in range(seqs):
        here = pl.ds(s * length, length)
        forget = f_acc[here, :].astype(BF).astype(F32)
        values = v_acc[here, :].astype(BF)
        gate = slack_ref[...] / (1.0 + jnp.exp(forget))
        damping = sum(
            lax.dot_general(t, spread, over_rows, preferred_element_type=F32)
            for t in three_terms(damp_ref[s])
        )
        decay = jnp.log(1.0 - gate) + damping
        within = sum(jnp.dot(later, t, preferred_element_type=F32) for t in three_terms(decay))
        weighted = (gate * jnp.exp(within)).astype(BF)
        total = within[:1, :] + decay[:1, :]
        for h in range(heads):
            cols = slice(h * head_dim, (h + 1) * head_dim)
            state = lax.dot_general(
                weighted[:, cols], values[:, cols], over_rows, preferred_element_type=F32
            )
            totals.append(total[:, cols])
            out_ref[:, s * heads + h] = state.astype(BF).reshape(parts, head_dim // parts, head_dim)
    pairs = seqs * heads
    terms = [t.astype(F32) for t in three_terms(jnp.concatenate(totals))]
    packed = jnp.concatenate([*terms, jnp.zeros((head_dim - 3 * pairs, head_dim), F32)])
    out_ref[:, pairs] = packed.T.astype(BF).reshape(parts, head_dim // parts, head_dim)


def states(pieces, plan, weights, sums, slack, damp, parts):
    seqs, heads, _ = damp.shape
    head_dim = weights[0].shape[1] // heads
    return in_vmem(
        functools.partial(state_kernel, plan=plan, head_dim=head_dim),
        jax.ShapeDtypeStruct((parts, seqs * heads + 1, head_dim // parts, head_dim), BF),
        *pieces,
        *weights,
        *sums,
        slack,
        damp,
        scratch=[pltpu.VMEM(s.shape, F32) for s in sums],
        flops=12 * len(pieces) * pieces[0].size * weights[0].shape[1],
    )


def combine_kernel(got_ref, query_ref, keys_ref, value_ref, cache_ref, read_ref):
    parts, pairs = got_ref.shape[0], got_ref.shape[1] - 1
    rows, head_dim = got_ref.shape[2:]
    after = jnp.zeros((rows, head_dim), F32)
    sums = [jnp.zeros((rows, head_dim), F32)] * pairs
    for src in range(parts - 1, -1, -1):
        scale = jnp.exp(after)
        for j in range(pairs):
            sums[j] = sums[j] + scale[:, j : j + 1] * got_ref[src, j].astype(F32)
        packed = got_ref[src, pairs].astype(F32)
        after = after + (
            packed
            + pltpu.roll(packed, head_dim - pairs, 1)
            + pltpu.roll(packed, head_dim - 2 * pairs, 1)
        )
    reads = []
    for j in range(pairs):
        rounded = sums[j].astype(BF)
        cache_ref[j] = rounded
        keys = keys_ref[:, j : j + 1]
        updated = (1.0 - keys) * rounded.astype(F32) + keys * value_ref[j : j + 1, :]
        reads.append(jnp.sum(query_ref[:, j : j + 1] * updated, axis=0, keepdims=True))
    reads = jnp.concatenate(reads)
    for p in range(parts):
        read_ref[p] = reads


def combine(got, query, keys, value):
    parts, tiles, rows, head_dim = got.shape
    return in_vmem(
        combine_kernel,
        [
            jax.ShapeDtypeStruct((tiles - 1, rows, head_dim), BF),
            jax.ShapeDtypeStruct((parts, tiles - 1, head_dim), F32),
        ],
        got,
        query,
        keys,
        value,
    )


def finish_kernel(got_ref, norm_ref, gate_ref, out_ref):
    heads = out_ref.shape[1] // got_ref.shape[2]
    head_dim = got_ref.shape[2]
    read = got_ref[0]
    for src in range(1, got_ref.shape[0]):
        read = read + got_ref[src]
    scaled = read * lax.rsqrt(jnp.mean(read * read, axis=1, keepdims=True) + 1e-06) * norm_ref[...]
    result = (scaled * gate_ref[...]).astype(BF)
    for s in range(out_ref.shape[0]):
        for h in range(heads):
            j = s * heads + h
            out_ref[s : s + 1, h * head_dim : (h + 1) * head_dim] = result[j : j + 1, :]


def new_token_kernel(x_ref, q_hbm, g_hbm, f_hbm, v_hbm, out_ref, x_here, rows, sems):
    seqs, slab = x_ref.shape
    here = pl.ds(pl.multiple_of(lax.axis_index("sp") * slab, slab), slab)
    sources = (q_hbm, g_hbm, f_hbm.at[here], v_hbm.at[here])
    copied([(w, rows.at[n]) for n, w in enumerate(sources)] + [(x_ref, x_here)], sems)
    for n in range(len(sources)):
        y = jnp.dot(x_here[...], rows[n], preferred_element_type=F32)
        for p in range(out_ref.shape[0]):
            out_ref[p, n * seqs : (n + 1) * seqs, :] = y


def prepare_kernel(got_ref, slack_ref, query_ref, keys_ref, value_ref, gate_ref):
    pairs, head_dim = value_ref.shape
    rows = query_ref.shape[0]
    seqs = got_ref.shape[1] // 4
    heads = pairs // seqs
    total = got_ref[0]
    for src in range(1, got_ref.shape[0]):
        total = total + got_ref[src]
    rounded = total.astype(BF).astype(F32)

    def by_head(x):
        return jnp.concatenate(
            [
                x[s : s + 1, h * head_dim : (h + 1) * head_dim]
                for s in range(x.shape[0])
                for h in range(heads)
            ]
        )

    query, gate, forget, value = (rounded[n * seqs : (n + 1) * seqs] for n in range(4))
    keys = slack_ref[...] * jax.nn.sigmoid(-forget)
    value_ref[...] = by_head(value)
    gate_ref[...] = by_head(gate * jax.nn.sigmoid(gate))
    own = lax.axis_index("sp") * rows + lax.broadcasted_iota(jnp.int32, (rows, head_dim), 0)
    chosen = jnp.where(lax.broadcasted_iota(jnp.int32, (rows, head_dim), 1) == own, 1.0, 0.0).astype(BF)

    def own_rows(x):
        return sum(
            lax.dot_general(chosen, t, (((1,), (1,)), ((), ())), preferred_element_type=F32)
            for t in three_terms(x)
        )

    query_ref[...] = own_rows(by_head(query))
    keys_ref[...] = own_rows(by_head(keys))


def per_device(
    tokens,
    first_token_input,
    forget_weight,
    value_weight,
    query_weight,
    output_gate_weight,
    forget_bound_slack,
    additional_damping_exponent,
    read_norm_scale,
):
    seqs, length, width = tokens.shape
    head_dim = read_norm_scale.shape[0]
    heads = additional_damping_exponent.shape[2]
    channels = heads * head_dim
    sp_count = lax.axis_size("sp")
    tp_count = lax.axis_size("tp")
    chips = tp_count // 2
    slack = forget_bound_slack.reshape(1, channels)

    def shifted(x, by):
        pairs = [(2 * c + k, 2 * ((c + by) % chips) + k) for c in range(chips) for k in (0, 1)]
        return lax.ppermute(x, "tp", pairs)

    def sibling(x):
        return lax.ppermute(x, "tp", [(i, i ^ 1) for i in range(tp_count)])

    def exchange(x):
        return lax.all_to_all(x, "sp", 0, 0, tiled=True)

    rows = seqs // 2 * length
    own_a, own_b = (x.reshape(rows, width) for x in split(tokens, 2))
    right_a, left_a = shifted(own_a, 1), shifted(own_a, -1)
    right_b, left_b = shifted(own_b, 1), shifted(own_b, -1)
    other_a, other_b = sibling(own_a), sibling(own_b)

    partial = in_vmem(
        new_token_kernel,
        jax.ShapeDtypeStruct((sp_count, 4 * seqs, channels), F32),
        *(
            pltpu.with_memory_space_constraint(x, pltpu.HBM)
            for x in (
                first_token_input,
                query_weight,
                output_gate_weight,
                forget_weight,
                value_weight,
            )
        ),
        in_specs=[pl.BlockSpec(memory_space=pltpu.HBM)] * 5,
        scratch=[
            pltpu.VMEM(first_token_input.shape, BF),
            pltpu.VMEM((4, *query_weight.shape), BF),
            pltpu.SemaphoreType.DMA((5,)),
        ],
    )
    new_sums = exchange(partial)
    row_count = head_dim // sp_count
    pairs = seqs * heads
    query_rows, key_rows, value_new, gate_new = in_vmem(
        prepare_kernel,
        [jax.ShapeDtypeStruct((row_count, pairs), F32)] * 2
        + [jax.ShapeDtypeStruct((pairs, head_dim), F32)] * 2,
        new_sums,
        slack,
    )

    far_a, far_b = shifted(right_a, 1), shifted(left_b, -1)
    other_right_a, other_left_a = sibling(right_a), sibling(left_a)
    other_right_b, other_left_b = sibling(right_b), sibling(left_b)
    other_far_a, other_far_b = sibling(far_a), sibling(far_b)

    def both(by):
        return ((by, False), (by, True))

    weights, sums = load_and_project(
        [own_a, other_a, own_b, other_b], (both(0), both(0)), (forget_weight, value_weight)
    )
    pieces = [right_a, other_right_a, left_b, other_left_b]
    sums = project(pieces, (both(1), both(-1)), weights, sums)
    pieces = [left_a, other_left_a, right_b, other_right_b]
    sums = project(pieces, (both(-1), both(1)), weights, sums)
    out = states(
        [far_a, other_far_a, far_b, other_far_b],
        (both(2), both(2)),
        weights,
        sums,
        slack,
        additional_damping_exponent.transpose(0, 2, 1),
        sp_count,
    )
    got = exchange(out)
    cache, read = combine(got, query_rows, key_rows, value_new)
    got = exchange(read)
    first_read = in_vmem(
        finish_kernel,
        jax.ShapeDtypeStruct((seqs, channels), BF),
        got,
        read_norm_scale.reshape(1, head_dim),
        gate_new,
    )
    return cache.reshape(seqs, heads, row_count, head_dim), first_read


def solution(mesh):
    placed = (
        P("gr", "sp", "tp"),
        P("gr", "sp"),
        P(None, "tp"),
        P(None, "tp"),
        P("sp", "tp"),
        P("sp", "tp"),
        P("tp"),
        P("gr", "sp", "tp"),
        P(),
    )

    return jax.shard_map(
        per_device,
        mesh=mesh,
        in_specs=placed,
        out_specs=(P("gr", "tp", "sp", None), P("gr", "tp")),
        check_vma=False,
    )
```

```python
import functools

import jax
import jax.numpy as jnp
from jax import lax
from jax.experimental import pallas as pl
from jax.experimental.pallas import tpu as pltpu
from jax.sharding import PartitionSpec as P


BF = jnp.bfloat16
F32 = jnp.float32


def three_terms(x):
    high = x.astype(BF)
    rest = x - high.astype(F32)
    middle = rest.astype(BF)
    low = (rest - middle.astype(F32)).astype(BF)
    return high, middle, low


VMEM = pl.BlockSpec(memory_space=pltpu.VMEM)


def in_vmem(kernel, out_shape, *arrays, in_specs=None, scratch=(), flops=0):
    return pl.pallas_call(
        kernel,
        in_specs=in_specs or [VMEM] * len(arrays),
        out_specs=jax.tree.map(lambda _: VMEM, out_shape),
        out_shape=out_shape,
        scratch_shapes=scratch,
        compiler_params=pltpu.CompilerParams(vmem_limit_bytes=12 << 20),
        cost_estimate=pl.CostEstimate(flops=flops, transcendentals=0, bytes_accessed=0),
    )(*arrays)


def copied(pairs, sems):
    copies = [pltpu.make_async_copy(*pair, sems.at[n]) for n, pair in enumerate(pairs)]
    for copy in copies:
        copy.start()
    for copy in copies:
        copy.wait()


def from_hbm(kernel, shapes, *arrays):
    return pl.pallas_call(
        kernel,
        in_specs=[pl.BlockSpec(memory_space=pltpu.HBM)] * len(arrays),
        out_specs=[VMEM] * len(shapes),
        out_shape=[pltpu.VMEM(shape, BF) for shape in shapes],
        scratch_shapes=[pltpu.SemaphoreType.DMA((len(shapes),))],
        compiler_params=pltpu.CompilerParams(vmem_limit_bytes=1 << 20),
    )(*(pltpu.with_memory_space_constraint(a, pltpu.HBM) for a in arrays))


def split_kernel(tokens_ref, *refs):
    seqs = tokens_ref.shape[0] // (len(refs) - 1)
    copied(
        [(tokens_ref.at[pl.ds(n * seqs, seqs)], out) for n, out in enumerate(refs[:-1])], refs[-1]
    )


def split(tokens, count):
    shape = (tokens.shape[0] // count, *tokens.shape[1:])
    return from_hbm(split_kernel, [shape] * count, tokens)


def block_of(tp, by, other):
    count = lax.axis_size("tp")
    return lax.rem((tp ^ 1 if other else tp) + count - 2 * by, count)


def products(pieces, sources, w_ref):
    tp = lax.axis_index("tp")
    total = None
    for piece, source in zip(pieces, sources):
        width = piece.shape[1]
        start = pl.multiple_of(block_of(tp, *source) * width, width)
        part = jnp.dot(piece[...], w_ref[pl.ds(start, width), :], preferred_element_type=F32)
        total = part if total is None else total + part
    return total


def add_products(pieces, plan, weights, sums, outs):
    rows = pieces[0].shape[0]
    for half, sources in enumerate(plan):
        here = pl.ds(half * rows, rows)
        some, pieces = pieces[: len(sources)], pieces[len(sources) :]
        for n, (w_ref, out) in enumerate(zip(weights, outs)):
            result = products(some, sources, w_ref)
            out[here, :] = sums[n][here, :] + result if sums else result


def project_kernel(*refs, plan):
    count = sum(map(len, plan))
    add_products(refs[:count], plan, refs[count : count + 2], refs[-4:-2], refs[-2:])


def project(pieces, plan, weights, sums):
    return in_vmem(
        functools.partial(project_kernel, plan=plan),
        [jax.ShapeDtypeStruct(s.shape, F32) for s in sums],
        *pieces,
        *weights,
        *sums,
        flops=4 * len(pieces) * pieces[0].size * weights[0].shape[1],
    )


def load_kernel(*refs, plan):
    count = sum(map(len, plan))
    pieces, (wf_hbm, wv_hbm, wf_ref, wv_ref, *outs, sems) = refs[:count], refs[count:]
    chips = lax.axis_size("tp") // 2
    depth = wf_ref.shape[0] // chips
    chip = lax.axis_index("tp") // 2
    copies = []
    for step in range(chips):
        here = pl.ds(pl.multiple_of(lax.rem(chip + step, chips) * depth, depth), depth)
        for n, (source, target) in enumerate(((wf_hbm, wf_ref), (wv_hbm, wv_ref))):
            copies.append(
                pltpu.make_async_copy(source.at[here], target.at[here], sems.at[2 * step + n])
            )
    for copy in copies:
        copy.start()
    for copy in copies[:2]:
        copy.wait()
    add_products(pieces, plan, (wf_ref, wv_ref), (), outs)
    for copy in copies[2:]:
        copy.wait()


def load_and_project(pieces, plan, weights):
    rows = len(plan) * pieces[0].shape[0]
    out = jax.ShapeDtypeStruct((rows, weights[0].shape[1]), F32)
    *weights, f, v = pl.pallas_call(
        functools.partial(load_kernel, plan=plan),
        in_specs=[VMEM] * len(pieces) + [pl.BlockSpec(memory_space=pltpu.HBM)] * 2,
        out_specs=[VMEM] * 4,
        out_shape=[pltpu.VMEM(w.shape, BF) for w in weights] + [out] * 2,
        scratch_shapes=[pltpu.SemaphoreType.DMA((lax.axis_size("tp"),))],
        compiler_params=pltpu.CompilerParams(vmem_limit_bytes=12 << 20),
        name="load",
    )(*pieces, *(pltpu.with_memory_space_constraint(w, pltpu.HBM) for w in weights))
    return [pltpu.with_memory_space_constraint(w, pltpu.VMEM) for w in weights], [f, v]


def state_kernel(*refs, plan, head_dim):
    count = sum(map(len, plan))
    pieces, (wf_ref, wv_ref, f_in, v_in, *refs) = refs[:count], refs[count:]
    slack_ref, damp_ref, out_ref, f_acc, v_acc = refs
    add_products(pieces, plan, (wf_ref, wv_ref), (f_in, v_in), (f_acc, v_acc))
    parts = out_ref.shape[0]
    seqs, heads, length = damp_ref.shape
    channels = heads * head_dim
    tall = length + 8
    row = lax.broadcasted_iota(jnp.int32, (tall, length), 0)
    column = lax.broadcasted_iota(jnp.int32, (tall, length), 1)
    later = jnp.where((column > row) | (row >= length), 1.0, 0.0).astype(BF)
    head = lax.broadcasted_iota(jnp.int32, (3 * heads, channels), 0) % heads
    channel = lax.broadcasted_iota(jnp.int32, (3 * heads, channels), 1)
    spread = jnp.where(channel // head_dim == head, 1.0, 0.0).astype(BF)
    over_rows = (((0,), (0,)), ((), ()))
    over_columns = (((1,), (1,)), ((), ()))
    totals = []
    for s in range(seqs):
        here = pl.ds(s * length, length)
        forget = f_acc[here, :].astype(BF).astype(F32)
        values = v_acc[here, :].astype(BF)
        gate = slack_ref[...] / (1.0 + jnp.exp(forget))
        high, middle, _ = three_terms(jnp.log(1.0 - gate))
        damping = lax.dot_general(
            later,
            jnp.concatenate(three_terms(damp_ref[s])),
            over_columns,
            preferred_element_type=F32,
        )
        damping = damping[:, :heads] + damping[:, heads : 2 * heads] + damping[:, 2 * heads :]
        sums = jnp.dot(
            jnp.concatenate([later, *three_terms(damping)], axis=1),
            jnp.concatenate([high, spread]),
            preferred_element_type=F32,
        ) + jnp.dot(later, middle, preferred_element_type=F32)
        weighted = (gate * jnp.exp(sums[:length])).astype(BF)
        for h in range(heads):
            cols = slice(h * head_dim, (h + 1) * head_dim)
            state = lax.dot_general(
                weighted[:, cols], values[:, cols], over_rows, preferred_element_type=F32
            )
            totals.append(sums[length : length + 1, cols])
            out_ref[:, s * heads + h] = state.astype(BF).reshape(parts, head_dim // parts, head_dim)
    pairs = seqs * heads
    terms = [t.astype(F32) for t in three_terms(jnp.concatenate(totals))]
    packed = jnp.concatenate([*terms, jnp.zeros((head_dim - 3 * pairs, head_dim), F32)])
    out_ref[:, pairs] = packed.T.astype(BF).reshape(parts, head_dim // parts, head_dim)


def states(pieces, plan, weights, sums, slack, damp, parts):
    seqs, heads, _ = damp.shape
    head_dim = weights[0].shape[1] // heads
    return in_vmem(
        functools.partial(state_kernel, plan=plan, head_dim=head_dim),
        jax.ShapeDtypeStruct((parts, seqs * heads + 1, head_dim // parts, head_dim), BF),
        *pieces,
        *weights,
        *sums,
        slack,
        damp,
        scratch=[pltpu.VMEM(s.shape, F32) for s in sums],
        flops=12 * len(pieces) * pieces[0].size * weights[0].shape[1],
    )


def combine_kernel(got_ref, query_ref, keys_ref, value_ref, cache_ref, read_ref):
    parts, pairs = got_ref.shape[0], got_ref.shape[1] - 1
    rows, head_dim = got_ref.shape[2:]
    after = jnp.zeros((rows, head_dim), F32)
    sums = [jnp.zeros((rows, head_dim), F32)] * pairs
    for src in range(parts - 1, -1, -1):
        scale = jnp.exp(after)
        for j in range(pairs):
            sums[j] = sums[j] + scale[:, j : j + 1] * got_ref[src, j].astype(F32)
        packed = got_ref[src, pairs].astype(F32)
        after = after + (
            packed
            + pltpu.roll(packed, head_dim - pairs, 1)
            + pltpu.roll(packed, head_dim - 2 * pairs, 1)
        )
    reads = []
    for j in range(pairs):
        rounded = sums[j].astype(BF)
        cache_ref[j] = rounded
        keys = keys_ref[:, j : j + 1]
        updated = (1.0 - keys) * rounded.astype(F32) + keys * value_ref[j : j + 1, :]
        reads.append(jnp.sum(query_ref[:, j : j + 1] * updated, axis=0, keepdims=True))
    reads = jnp.concatenate(reads)
    for p in range(parts):
        read_ref[p] = reads


def combine(got, query, keys, value):
    parts, tiles, rows, head_dim = got.shape
    return in_vmem(
        combine_kernel,
        [
            pltpu.VMEM((tiles - 1, rows, head_dim), BF),
            jax.ShapeDtypeStruct((parts, tiles - 1, head_dim), F32),
        ],
        got,
        query,
        keys,
        value,
    )


def finish_kernel(got_ref, norm_ref, gate_ref, out_ref):
    heads = out_ref.shape[1] // got_ref.shape[2]
    head_dim = got_ref.shape[2]
    read = got_ref[0]
    for src in range(1, got_ref.shape[0]):
        read = read + got_ref[src]
    scaled = read * lax.rsqrt(jnp.mean(read * read, axis=1, keepdims=True) + 1e-06) * norm_ref[...]
    result = (scaled * gate_ref[...]).astype(BF)
    for s in range(out_ref.shape[0]):
        for h in range(heads):
            j = s * heads + h
            out_ref[s : s + 1, h * head_dim : (h + 1) * head_dim] = result[j : j + 1, :]


def new_token_kernel(x_ref, q_hbm, g_hbm, f_hbm, v_hbm, out_ref, x_here, rows, sems):
    seqs, slab = x_ref.shape
    here = pl.ds(pl.multiple_of(lax.axis_index("sp") * slab, slab), slab)
    sources = (q_hbm, g_hbm, f_hbm.at[here], v_hbm.at[here])
    copied([(w, rows.at[n]) for n, w in enumerate(sources)] + [(x_ref, x_here)], sems)
    for n in range(len(sources)):
        y = jnp.dot(x_here[...], rows[n], preferred_element_type=F32)
        for p in range(out_ref.shape[0]):
            out_ref[p, n * seqs : (n + 1) * seqs, :] = y


def prepare_kernel(got_ref, slack_ref, query_ref, keys_ref, value_ref, gate_ref):
    pairs, head_dim = value_ref.shape
    rows = query_ref.shape[0]
    seqs = got_ref.shape[1] // 4
    heads = pairs // seqs
    total = got_ref[0]
    for src in range(1, got_ref.shape[0]):
        total = total + got_ref[src]
    rounded = total.astype(BF).astype(F32)

    def by_head(x):
        return jnp.concatenate(
            [
                x[s : s + 1, h * head_dim : (h + 1) * head_dim]
                for s in range(x.shape[0])
                for h in range(heads)
            ]
        )

    query, gate, forget, value = (rounded[n * seqs : (n + 1) * seqs] for n in range(4))
    keys = slack_ref[...] * jax.nn.sigmoid(-forget)
    value_ref[...] = by_head(value)
    gate_ref[...] = by_head(gate * jax.nn.sigmoid(gate))
    own = lax.axis_index("sp") * rows + lax.broadcasted_iota(jnp.int32, (rows, head_dim), 0)
    chosen = jnp.where(lax.broadcasted_iota(jnp.int32, (rows, head_dim), 1) == own, 1.0, 0.0).astype(BF)

    def own_rows(x):
        return sum(
            lax.dot_general(chosen, t, (((1,), (1,)), ((), ())), preferred_element_type=F32)
            for t in three_terms(x)
        )

    query_ref[...] = own_rows(by_head(query))
    keys_ref[...] = own_rows(by_head(keys))


def per_device(
    tokens,
    first_token_input,
    forget_weight,
    value_weight,
    query_weight,
    output_gate_weight,
    forget_bound_slack,
    additional_damping_exponent,
    read_norm_scale,
):
    seqs, length, width = tokens.shape
    head_dim = read_norm_scale.shape[0]
    heads = additional_damping_exponent.shape[2]
    channels = heads * head_dim
    sp_count = lax.axis_size("sp")
    tp_count = lax.axis_size("tp")
    chips = tp_count // 2
    slack = forget_bound_slack.reshape(1, channels)

    def shifted(x, by):
        pairs = [(2 * c + k, 2 * ((c + by) % chips) + k) for c in range(chips) for k in (0, 1)]
        return lax.ppermute(x, "tp", pairs)

    def sibling(x):
        return lax.ppermute(x, "tp", [(i, i ^ 1) for i in range(tp_count)])

    def exchange(x):
        return lax.all_to_all(x, "sp", 0, 0, tiled=True)

    rows = seqs // 2 * length
    own_a, own_b = (x.reshape(rows, width) for x in split(tokens, 2))
    right_a, left_a = shifted(own_a, 1), shifted(own_a, -1)
    right_b, left_b = shifted(own_b, 1), shifted(own_b, -1)
    other_a, other_b = sibling(own_a), sibling(own_b)

    partial = in_vmem(
        new_token_kernel,
        jax.ShapeDtypeStruct((sp_count, 4 * seqs, channels), F32),
        *(
            pltpu.with_memory_space_constraint(x, pltpu.HBM)
            for x in (
                first_token_input,
                query_weight,
                output_gate_weight,
                forget_weight,
                value_weight,
            )
        ),
        in_specs=[pl.BlockSpec(memory_space=pltpu.HBM)] * 5,
        scratch=[
            pltpu.VMEM(first_token_input.shape, BF),
            pltpu.VMEM((4, *query_weight.shape), BF),
            pltpu.SemaphoreType.DMA((5,)),
        ],
    )
    new_sums = exchange(partial)
    row_count = head_dim // sp_count
    pairs = seqs * heads
    query_rows, key_rows, value_new, gate_new = in_vmem(
        prepare_kernel,
        [jax.ShapeDtypeStruct((row_count, pairs), F32)] * 2
        + [jax.ShapeDtypeStruct((pairs, head_dim), F32)] * 2,
        new_sums,
        slack,
    )

    far_a, far_b = shifted(right_a, 1), shifted(left_b, -1)
    other_right_a, other_left_a = sibling(right_a), sibling(left_a)
    other_right_b, other_left_b = sibling(right_b), sibling(left_b)
    other_far_a, other_far_b = sibling(far_a), sibling(far_b)

    def both(by):
        return ((by, False), (by, True))

    weights, sums = load_and_project(
        [own_a, other_a, own_b, other_b], (both(0), both(0)), (forget_weight, value_weight)
    )
    pieces = [right_a, other_right_a, left_a, other_left_a]
    pieces += [right_b, other_right_b, left_b, other_left_b]
    sums = project(pieces, (both(1) + both(-1), both(1) + both(-1)), weights, sums)
    out = states(
        [far_a, other_far_a, far_b, other_far_b],
        (both(2), both(2)),
        weights,
        sums,
        slack,
        additional_damping_exponent.transpose(0, 2, 1),
        sp_count,
    )
    got = exchange(out)
    cache, read = combine(got, query_rows, key_rows, value_new)
    got = exchange(read)
    first_read = in_vmem(
        finish_kernel,
        jax.ShapeDtypeStruct((seqs, channels), BF),
        got,
        read_norm_scale.reshape(1, head_dim),
        gate_new,
    )
    return cache.reshape(seqs, heads, row_count, head_dim), first_read


def solution(mesh):
    placed = (
        P("gr", "sp", "tp"),
        P("gr", "sp"),
        P(None, "tp"),
        P(None, "tp"),
        P("sp", "tp"),
        P("sp", "tp"),
        P("tp"),
        P("gr", "sp", "tp"),
        P(),
    )

    return jax.shard_map(
        per_device,
        mesh=mesh,
        in_specs=placed,
        out_specs=(P("gr", "tp", "sp", None), P("gr", "tp")),
        check_vma=False,
    )
```

```python
import functools

import jax
import jax.numpy as jnp
from jax import lax
from jax.experimental import pallas as pl
from jax.experimental.pallas import tpu as pltpu
from jax.sharding import PartitionSpec as P


BF = jnp.bfloat16
F32 = jnp.float32
NEAR = 4


def three_terms(x):
    high = x.astype(BF)
    rest = x - high.astype(F32)
    middle = rest.astype(BF)
    low = (rest - middle.astype(F32)).astype(BF)
    return high, middle, low


VMEM = pl.BlockSpec(memory_space=pltpu.VMEM)


def in_vmem(kernel, out_shape, *arrays, in_specs=None, scratch=(), flops=0):
    return pl.pallas_call(
        kernel,
        in_specs=in_specs or [VMEM] * len(arrays),
        out_specs=jax.tree.map(lambda _: VMEM, out_shape),
        out_shape=out_shape,
        scratch_shapes=scratch,
        compiler_params=pltpu.CompilerParams(vmem_limit_bytes=12 << 20),
        cost_estimate=pl.CostEstimate(flops=flops, transcendentals=0, bytes_accessed=0),
    )(*arrays)


def copied(pairs, sems):
    copies = [pltpu.make_async_copy(*pair, sems.at[n]) for n, pair in enumerate(pairs)]
    for copy in copies:
        copy.start()
    for copy in copies:
        copy.wait()


def from_hbm(kernel, shapes, *arrays):
    return pl.pallas_call(
        kernel,
        in_specs=[pl.BlockSpec(memory_space=pltpu.HBM)] * len(arrays),
        out_specs=[VMEM] * len(shapes),
        out_shape=[pltpu.VMEM(shape, BF) for shape in shapes],
        scratch_shapes=[pltpu.SemaphoreType.DMA((len(shapes),))],
        compiler_params=pltpu.CompilerParams(vmem_limit_bytes=1 << 20),
    )(*(pltpu.with_memory_space_constraint(a, pltpu.HBM) for a in arrays))


def split_kernel(tokens_ref, *refs):
    seqs = tokens_ref.shape[0] // (len(refs) - 1)
    copied(
        [(tokens_ref.at[pl.ds(n * seqs, seqs)], out) for n, out in enumerate(refs[:-1])], refs[-1]
    )


def split(tokens, count):
    shape = (tokens.shape[0] // count, *tokens.shape[1:])
    return from_hbm(split_kernel, [shape] * count, tokens)


def block_of(tp, by, other):
    count = lax.axis_size("tp")
    return lax.rem((tp ^ 1 if other else tp) + count - 2 * by, count)


def products(pieces, sources, w_ref):
    tp = lax.axis_index("tp")
    total = None
    for piece, source in zip(pieces, sources):
        width = piece.shape[1]
        start = pl.multiple_of(block_of(tp, *source) * width, width)
        part = jnp.dot(piece[...], w_ref[pl.ds(start, width), :], preferred_element_type=F32)
        total = part if total is None else total + part
    return total


def add_products(pieces, plan, weights, sums, outs):
    rows = pieces[0].shape[0]
    for half, sources in enumerate(plan):
        here = pl.ds(half * rows, rows)
        some, pieces = pieces[: len(sources)], pieces[len(sources) :]
        for n, (w_ref, out) in enumerate(zip(weights, outs)):
            result = products(some, sources, w_ref)
            out[here, :] = sums[n][here, :] + result if sums else result


def project_kernel(*refs, plan):
    count = sum(map(len, plan))
    add_products(refs[:count], plan, refs[count : count + 2], refs[-4:-2], refs[-2:])


def project(pieces, plan, weights, sums):
    return in_vmem(
        functools.partial(project_kernel, plan=plan),
        [jax.ShapeDtypeStruct(s.shape, F32) for s in sums],
        *pieces,
        *weights,
        *sums,
        flops=4 * len(pieces) * pieces[0].size * weights[0].shape[1],
    )


def load_kernel(*refs, plan):
    count = sum(map(len, plan))
    pieces, (wf_hbm, wv_hbm, wf_ref, wv_ref, *outs, sems) = refs[:count], refs[count:]
    chips = lax.axis_size("tp") // 2
    depth = wf_ref.shape[0] // chips
    chip = lax.axis_index("tp") // 2
    copies = []
    for step in range(chips):
        here = pl.ds(pl.multiple_of(lax.rem(chip + step, chips) * depth, depth), depth)
        for n, (source, target) in enumerate(((wf_hbm, wf_ref), (wv_hbm, wv_ref))):
            copies.append(
                pltpu.make_async_copy(source.at[here], target.at[here], sems.at[2 * step + n])
            )
    for copy in copies:
        copy.start()
    for copy in copies[:2]:
        copy.wait()
    add_products(pieces, plan, (wf_ref, wv_ref), (), outs)
    for copy in copies[2:]:
        copy.wait()


def load_and_project(pieces, plan, weights):
    rows = len(plan) * pieces[0].shape[0]
    out = jax.ShapeDtypeStruct((rows, weights[0].shape[1]), F32)
    *weights, f, v = pl.pallas_call(
        functools.partial(load_kernel, plan=plan),
        in_specs=[VMEM] * len(pieces) + [pl.BlockSpec(memory_space=pltpu.HBM)] * 2,
        out_specs=[VMEM] * 4,
        out_shape=[pltpu.VMEM(w.shape, BF) for w in weights] + [out] * 2,
        scratch_shapes=[pltpu.SemaphoreType.DMA((lax.axis_size("tp"),))],
        compiler_params=pltpu.CompilerParams(vmem_limit_bytes=12 << 20),
        name="load",
    )(*pieces, *(pltpu.with_memory_space_constraint(w, pltpu.HBM) for w in weights))
    return [pltpu.with_memory_space_constraint(w, pltpu.VMEM) for w in weights], [f, v]


def state_kernel(*refs, plan, head_dim):
    count = sum(map(len, plan))
    pieces, (wf_ref, wv_ref, f_in, v_in, *refs) = refs[:count], refs[count:]
    slack_ref, damp_ref, *outs, total_ref, state_ref, f_acc, v_acc, parts_ref = refs
    add_products(pieces, plan, (wf_ref, wv_ref), (f_in, v_in), (f_acc, v_acc))
    far, rows = parts_ref.shape[1], parts_ref.shape[3]
    seqs, heads, length = damp_ref.shape
    channels = heads * head_dim
    tall = length + 8
    row = lax.broadcasted_iota(jnp.int32, (tall, length), 0)
    column = lax.broadcasted_iota(jnp.int32, (tall, length), 1)
    later = jnp.where((column > row) | (row >= length), 1.0, 0.0).astype(BF)
    head = lax.broadcasted_iota(jnp.int32, (3 * heads, channels), 0) % heads
    channel = lax.broadcasted_iota(jnp.int32, (3 * heads, channels), 1)
    spread = jnp.where(channel // head_dim == head, 1.0, 0.0).astype(BF)
    over_rows = (((0,), (0,)), ((), ()))
    over_columns = (((1,), (1,)), ((), ()))
    totals = []
    for s in range(seqs):
        here = pl.ds(s * length, length)
        forget = f_acc[here, :].astype(BF).astype(F32)
        values = v_acc[here, :].astype(BF)
        gate = slack_ref[...] / (1.0 + jnp.exp(forget))
        high, middle, _ = three_terms(jnp.log(1.0 - gate))
        damping = lax.dot_general(
            later,
            jnp.concatenate(three_terms(damp_ref[s])),
            over_columns,
            preferred_element_type=F32,
        )
        damping = damping[:, :heads] + damping[:, heads : 2 * heads] + damping[:, 2 * heads :]
        sums = jnp.dot(
            jnp.concatenate([later, *three_terms(damping)], axis=1),
            jnp.concatenate([high, spread]),
            preferred_element_type=F32,
        ) + jnp.dot(later, middle, preferred_element_type=F32)
        weighted = (gate * jnp.exp(sums[:length])).astype(BF)
        for h in range(heads):
            cols = slice(h * head_dim, (h + 1) * head_dim)
            state = lax.dot_general(
                weighted[:, cols], values[:, cols], over_rows, preferred_element_type=F32
            )
            totals.append(sums[length : length + 1, cols])
            state = state.astype(BF)
            state_ref[s * heads + h] = state
            blocks = state.reshape(far, NEAR, rows, head_dim)
            for y in range(NEAR):
                parts_ref[y, :, s * heads + h] = blocks[:, y]
    pairs = seqs * heads
    totals = jnp.concatenate(totals)
    for p in range(total_ref.shape[0]):
        total_ref[p] = totals
    terms = [t.astype(F32) for t in three_terms(totals)]
    packed = jnp.concatenate([*terms, jnp.zeros((head_dim - 3 * pairs, head_dim), F32)])
    blocks = packed.T.astype(BF).reshape(far, NEAR, rows, head_dim)
    for y in range(NEAR):
        parts_ref[y, :, pairs] = blocks[:, y]
    near = lax.rem(lax.axis_index("sp"), NEAR)
    for step, out in enumerate(outs):
        out[...] = parts_ref[lax.rem(near + step, NEAR)]


def states(pieces, plan, weights, sums, slack, damp, parts):
    seqs, heads, _ = damp.shape
    head_dim = weights[0].shape[1] // heads
    pairs = seqs * heads
    shape = (parts // NEAR, pairs + 1, head_dim // parts, head_dim)
    *outs, totals, state = in_vmem(
        functools.partial(state_kernel, plan=plan, head_dim=head_dim),
        [jax.ShapeDtypeStruct(shape, BF)] * NEAR
        + [
            jax.ShapeDtypeStruct((parts, pairs, head_dim), F32),
            jax.ShapeDtypeStruct((pairs, head_dim, head_dim), BF),
        ],
        *pieces,
        *weights,
        *sums,
        slack,
        damp,
        scratch=[pltpu.VMEM(s.shape, F32) for s in sums] + [pltpu.VMEM((NEAR, *shape), BF)],
        flops=12 * len(pieces) * pieces[0].size * weights[0].shape[1],
    )
    return outs, totals, state


def unpacked(tile, pairs):
    tile = tile.astype(F32)
    lanes = tile.shape[1]
    return tile + pltpu.roll(tile, lanes - pairs, 1) + pltpu.roll(tile, lanes - 2 * pairs, 1)


def joined(tiles, place, count):
    pairs = tiles[0].shape[0] - 1
    places = [lax.rem(place + count - step, count) for step in range(count)]
    totals = [unpacked(tile[pairs], pairs) for tile in tiles]
    sums = [None] * pairs
    for here, tile in zip(places, tiles):
        after = sum(jnp.where(p > here, 1.0, 0.0) * total for p, total in zip(places, totals))
        scale = jnp.exp(after)
        for j in range(pairs):
            part = scale[:, j : j + 1] * tile[j].astype(F32)
            sums[j] = part if sums[j] is None else sums[j] + part
    return sums, sum(totals)


def near_kernel(*refs):
    tiles, outs, parts_ref = refs[:NEAR], refs[NEAR:-1], refs[-1]
    far, tile_count, rows, lanes = parts_ref.shape
    pairs = tile_count - 1
    me = lax.axis_index("sp")
    lane = lax.broadcasted_iota(jnp.int32, (rows, lanes), 1)
    for z in range(far):
        sums, total = joined([t.at[z] for t in tiles], lax.rem(me, NEAR), NEAR)
        for j in range(pairs):
            parts_ref[z, j] = sums[j].astype(BF)
        high, middle, low = (t.astype(F32) for t in three_terms(total))
        packed = jnp.where(lane < 2 * pairs, pltpu.roll(middle, pairs, 1), pltpu.roll(low, 2 * pairs, 1))
        packed = jnp.where(lane < pairs, high, packed)
        parts_ref[z, pairs] = jnp.where(lane < 3 * pairs, packed, 0.0).astype(BF)
    for step, out in enumerate(outs):
        out[...] = parts_ref[lax.rem(me // NEAR + step, far)]


def join_near(tiles):
    shape = tiles[0].shape
    return in_vmem(
        near_kernel,
        [jax.ShapeDtypeStruct(shape[1:], BF)] * shape[0],
        *tiles,
        scratch=[pltpu.VMEM(shape, BF)],
    )


def far_kernel(*refs):
    tiles, cache_ref = refs[:-1], refs[-1]
    sums, _ = joined(tiles, lax.axis_index("sp") // NEAR, len(tiles))
    for j, part in enumerate(sums):
        cache_ref[j] = part.astype(BF)


def join_far(tiles):
    tile_count, rows, lanes = tiles[0].shape
    return in_vmem(far_kernel, pltpu.VMEM((tile_count - 1, rows, lanes), BF), *tiles)


def read_kernel(totals_ref, state_ref, query_ref, keys_ref, out_ref):
    me = lax.axis_index("sp")
    after = sum(
        jnp.where(src > me, 1.0, 0.0) * totals_ref[src] for src in range(totals_ref.shape[0])
    )
    weights = query_ref[...] * (1.0 - keys_ref[...]) * jnp.exp(after)
    pairs = weights.shape[0]
    terms = jnp.concatenate(three_terms(weights))
    reads = []
    for j in range(pairs):
        parts = jnp.dot(terms, state_ref[j], preferred_element_type=F32)
        reads.append(sum(parts[n : n + 1, :] for n in range(j, 3 * pairs, pairs)))
    reads = jnp.concatenate(reads)
    for p in range(out_ref.shape[0]):
        out_ref[p] = reads


def read_parts(totals, state, query, keys):
    return in_vmem(read_kernel, jax.ShapeDtypeStruct(totals.shape, F32), totals, state, query, keys)


def finish_kernel(got_ref, query_ref, keys_ref, value_ref, norm_ref, gate_ref, out_ref):
    heads = out_ref.shape[1] // got_ref.shape[2]
    head_dim = got_ref.shape[2]
    shared = jnp.sum(query_ref[...] * keys_ref[...], axis=1, keepdims=True)
    read = shared * value_ref[...]
    for src in range(got_ref.shape[0]):
        read = read + got_ref[src]
    scaled = read * lax.rsqrt(jnp.mean(read * read, axis=1, keepdims=True) + 1e-06) * norm_ref[...]
    result = (scaled * gate_ref[...]).astype(BF)
    for s in range(out_ref.shape[0]):
        for h in range(heads):
            j = s * heads + h
            out_ref[s : s + 1, h * head_dim : (h + 1) * head_dim] = result[j : j + 1, :]


def new_token_kernel(x_ref, q_hbm, g_hbm, f_hbm, v_hbm, out_ref, x_here, rows, sems):
    seqs, slab = x_ref.shape
    here = pl.ds(pl.multiple_of(lax.axis_index("sp") * slab, slab), slab)
    sources = (q_hbm, g_hbm, f_hbm.at[here], v_hbm.at[here])
    copied([(w, rows.at[n]) for n, w in enumerate(sources)] + [(x_ref, x_here)], sems)
    for n in range(len(sources)):
        y = jnp.dot(x_here[...], rows[n], preferred_element_type=F32)
        for p in range(out_ref.shape[0]):
            out_ref[p, n * seqs : (n + 1) * seqs, :] = y


def prepare_kernel(got_ref, slack_ref, query_ref, keys_ref, value_ref, gate_ref):
    pairs, head_dim = value_ref.shape
    seqs = got_ref.shape[1] // 4
    heads = pairs // seqs
    total = got_ref[0]
    for src in range(1, got_ref.shape[0]):
        total = total + got_ref[src]
    rounded = total.astype(BF).astype(F32)

    def by_head(x):
        return jnp.concatenate(
            [
                x[s : s + 1, h * head_dim : (h + 1) * head_dim]
                for s in range(x.shape[0])
                for h in range(heads)
            ]
        )

    query, gate, forget, value = (rounded[n * seqs : (n + 1) * seqs] for n in range(4))
    keys = slack_ref[...] * jax.nn.sigmoid(-forget)
    value_ref[...] = by_head(value)
    gate_ref[...] = by_head(gate * jax.nn.sigmoid(gate))
    query_ref[...] = by_head(query)
    keys_ref[...] = by_head(keys)


def per_device(
    tokens,
    first_token_input,
    forget_weight,
    value_weight,
    query_weight,
    output_gate_weight,
    forget_bound_slack,
    additional_damping_exponent,
    read_norm_scale,
):
    seqs, length, width = tokens.shape
    head_dim = read_norm_scale.shape[0]
    heads = additional_damping_exponent.shape[2]
    channels = heads * head_dim
    sp_count = lax.axis_size("sp")
    tp_count = lax.axis_size("tp")
    chips = tp_count // 2
    slack = forget_bound_slack.reshape(1, channels)

    def shifted(x, by):
        pairs = [(2 * c + k, 2 * ((c + by) % chips) + k) for c in range(chips) for k in (0, 1)]
        return lax.ppermute(x, "tp", pairs)

    def sibling(x):
        return lax.ppermute(x, "tp", [(i, i ^ 1) for i in range(tp_count)])

    def exchange(x):
        return lax.all_to_all(x, "sp", 0, 0, tiled=True)

    rows = seqs // 2 * length
    own_a, own_b = (x.reshape(rows, width) for x in split(tokens, 2))
    right_a, left_a = shifted(own_a, 1), shifted(own_a, -1)
    right_b, left_b = shifted(own_b, 1), shifted(own_b, -1)
    other_a, other_b = sibling(own_a), sibling(own_b)

    partial = in_vmem(
        new_token_kernel,
        jax.ShapeDtypeStruct((sp_count, 4 * seqs, channels), F32),
        *(
            pltpu.with_memory_space_constraint(x, pltpu.HBM)
            for x in (
                first_token_input,
                query_weight,
                output_gate_weight,
                forget_weight,
                value_weight,
            )
        ),
        in_specs=[pl.BlockSpec(memory_space=pltpu.HBM)] * 5,
        scratch=[
            pltpu.VMEM(first_token_input.shape, BF),
            pltpu.VMEM((4, *query_weight.shape), BF),
            pltpu.SemaphoreType.DMA((5,)),
        ],
    )
    new_sums = exchange(partial)
    row_count = head_dim // sp_count
    pairs = seqs * heads
    query_new, keys_new, value_new, gate_new = in_vmem(
        prepare_kernel, [jax.ShapeDtypeStruct((pairs, head_dim), F32)] * 4, new_sums, slack
    )

    far_a, far_b = shifted(right_a, 1), shifted(left_b, -1)
    other_right_a, other_left_a = sibling(right_a), sibling(left_a)
    other_right_b, other_left_b = sibling(right_b), sibling(left_b)
    other_far_a, other_far_b = sibling(far_a), sibling(far_b)

    def both(by):
        return ((by, False), (by, True))

    weights, sums = load_and_project(
        [own_a, other_a, own_b, other_b], (both(0), both(0)), (forget_weight, value_weight)
    )
    pieces = [right_a, other_right_a, left_a, other_left_a]
    pieces += [right_b, other_right_b, left_b, other_left_b]
    sums = project(pieces, (both(1) + both(-1), both(1) + both(-1)), weights, sums)
    parts, totals, state = states(
        [far_a, other_far_a, far_b, other_far_b],
        (both(2), both(2)),
        weights,
        sums,
        slack,
        additional_damping_exponent.transpose(0, 2, 1),
        sp_count,
    )

    planes = sp_count // NEAR

    def along_y(step):
        pairs = [
            (z * NEAR + y, z * NEAR + (y + step) % NEAR) for z in range(planes) for y in range(NEAR)
        ]
        return lax.ppermute(parts[step], "sp", pairs)

    def along_z(step):
        pairs = [
            (z * NEAR + y, (z + step) % planes * NEAR + y)
            for z in range(planes)
            for y in range(NEAR)
        ]
        return lax.ppermute(parts[step], "sp", pairs)

    parts = [parts[0], *(along_y(step) for step in range(1, NEAR))]
    parts = join_near(parts)
    parts = [parts[0], *(along_z(step) for step in range(1, planes))]
    cache = join_far(parts)

    totals = exchange(totals)
    read = read_parts(totals, state, query_new, keys_new)
    got = exchange(read)
    first_read = in_vmem(
        finish_kernel,
        jax.ShapeDtypeStruct((seqs, channels), BF),
        got,
        query_new,
        keys_new,
        value_new,
        read_norm_scale.reshape(1, head_dim),
        gate_new,
    )
    return cache.reshape(seqs, heads, row_count, head_dim), first_read


def solution(mesh):
    placed = (
        P("gr", "sp", "tp"),
        P("gr", "sp"),
        P(None, "tp"),
        P(None, "tp"),
        P("sp", "tp"),
        P("sp", "tp"),
        P("tp"),
        P("gr", "sp", "tp"),
        P(),
    )

    return jax.shard_map(
        per_device,
        mesh=mesh,
        in_specs=placed,
        out_specs=(P("gr", "tp", "sp", None), P("gr", "tp")),
        check_vma=False,
    )
```

```python
import functools

import jax
import jax.numpy as jnp
from jax import lax
from jax.experimental import pallas as pl
from jax.experimental.pallas import tpu as pltpu
from jax.sharding import PartitionSpec as P


BF = jnp.bfloat16
F32 = jnp.float32
NEAR = 4


def three_terms(x):
    high = x.astype(BF)
    rest = x - high.astype(F32)
    middle = rest.astype(BF)
    low = (rest - middle.astype(F32)).astype(BF)
    return high, middle, low


VMEM = pl.BlockSpec(memory_space=pltpu.VMEM)


def in_vmem(kernel, out_shape, *arrays, in_specs=None, scratch=(), flops=0):
    return pl.pallas_call(
        kernel,
        in_specs=in_specs or [VMEM] * len(arrays),
        out_specs=jax.tree.map(lambda _: VMEM, out_shape),
        out_shape=out_shape,
        scratch_shapes=scratch,
        compiler_params=pltpu.CompilerParams(vmem_limit_bytes=12 << 20),
        cost_estimate=pl.CostEstimate(flops=flops, transcendentals=0, bytes_accessed=0),
    )(*arrays)


def copied(pairs, sems):
    copies = [pltpu.make_async_copy(*pair, sems.at[n]) for n, pair in enumerate(pairs)]
    for copy in copies:
        copy.start()
    for copy in copies:
        copy.wait()


def from_hbm(kernel, shapes, *arrays):
    return pl.pallas_call(
        kernel,
        in_specs=[pl.BlockSpec(memory_space=pltpu.HBM)] * len(arrays),
        out_specs=[VMEM] * len(shapes),
        out_shape=[pltpu.VMEM(shape, BF) for shape in shapes],
        scratch_shapes=[pltpu.SemaphoreType.DMA((len(shapes),))],
        compiler_params=pltpu.CompilerParams(vmem_limit_bytes=1 << 20),
    )(*(pltpu.with_memory_space_constraint(a, pltpu.HBM) for a in arrays))


def split_kernel(tokens_ref, *refs):
    seqs = tokens_ref.shape[0] // (len(refs) - 1)
    copied(
        [(tokens_ref.at[pl.ds(n * seqs, seqs)], out) for n, out in enumerate(refs[:-1])], refs[-1]
    )


def split(tokens, count):
    shape = (tokens.shape[0] // count, *tokens.shape[1:])
    return from_hbm(split_kernel, [shape] * count, tokens)


def block_of(tp, by, other):
    count = lax.axis_size("tp")
    return lax.rem((tp ^ 1 if other else tp) + count - 2 * by, count)


def products(pieces, sources, w_ref):
    tp = lax.axis_index("tp")
    total = None
    for piece, source in zip(pieces, sources):
        width = piece.shape[1]
        start = pl.multiple_of(block_of(tp, *source) * width, width)
        part = jnp.dot(piece[...], w_ref[pl.ds(start, width), :], preferred_element_type=F32)
        total = part if total is None else total + part
    return total


def add_products(pieces, plan, weights, sums, outs):
    rows = pieces[0].shape[0]
    for half, sources in enumerate(plan):
        here = pl.ds(half * rows, rows)
        some, pieces = pieces[: len(sources)], pieces[len(sources) :]
        for n, (w_ref, out) in enumerate(zip(weights, outs)):
            result = products(some, sources, w_ref)
            out[here, :] = sums[n][here, :] + result if sums else result


def project_kernel(*refs, plan):
    count = sum(map(len, plan))
    add_products(refs[:count], plan, refs[count : count + 2], refs[-4:-2], refs[-2:])


def project(pieces, plan, weights, sums):
    return in_vmem(
        functools.partial(project_kernel, plan=plan),
        [jax.ShapeDtypeStruct(s.shape, F32) for s in sums],
        *pieces,
        *weights,
        *sums,
        flops=4 * len(pieces) * pieces[0].size * weights[0].shape[1],
    )


def load_kernel(*refs, plan):
    count = sum(map(len, plan))
    pieces, (wf_hbm, wv_hbm, wf_ref, wv_ref, *outs, sems) = refs[:count], refs[count:]
    chips = lax.axis_size("tp") // 2
    depth = wf_ref.shape[0] // chips
    chip = lax.axis_index("tp") // 2
    copies = []
    for step in range(chips):
        here = pl.ds(pl.multiple_of(lax.rem(chip + step, chips) * depth, depth), depth)
        for n, (source, target) in enumerate(((wf_hbm, wf_ref), (wv_hbm, wv_ref))):
            copies.append(
                pltpu.make_async_copy(source.at[here], target.at[here], sems.at[2 * step + n])
            )
    for copy in copies:
        copy.start()
    for copy in copies[:2]:
        copy.wait()
    add_products(pieces, plan, (wf_ref, wv_ref), (), outs)
    for copy in copies[2:]:
        copy.wait()


def load_and_project(pieces, plan, weights):
    rows = len(plan) * pieces[0].shape[0]
    out = jax.ShapeDtypeStruct((rows, weights[0].shape[1]), F32)
    *weights, f, v = pl.pallas_call(
        functools.partial(load_kernel, plan=plan),
        in_specs=[VMEM] * len(pieces) + [pl.BlockSpec(memory_space=pltpu.HBM)] * 2,
        out_specs=[VMEM] * 4,
        out_shape=[pltpu.VMEM(w.shape, BF) for w in weights] + [out] * 2,
        scratch_shapes=[pltpu.SemaphoreType.DMA((lax.axis_size("tp"),))],
        compiler_params=pltpu.CompilerParams(vmem_limit_bytes=12 << 20),
        name="load",
    )(*pieces, *(pltpu.with_memory_space_constraint(w, pltpu.HBM) for w in weights))
    return [pltpu.with_memory_space_constraint(w, pltpu.VMEM) for w in weights], [f, v]


def gates(forget, slack):
    return slack / (1.0 + jnp.exp(forget.astype(F32)))


def total_kernel(*refs, plan):
    count = sum(map(len, plan))
    pieces, (wf_ref, wv_ref, f_in, v_in, *refs) = refs[:count], refs[count:]
    slack_ref, damp_ref, f_out, v_out, total_ref, f_acc, v_acc = refs
    add_products(pieces, plan, (wf_ref, wv_ref), (f_in, v_in), (f_acc, v_acc))
    seqs, heads, length = damp_ref.shape
    head_dim = total_ref.shape[2]
    totals = []
    for s in range(seqs):
        here = pl.ds(s * length, length)
        forget = f_acc[here, :].astype(BF)
        f_out[here, :] = forget
        v_out[here, :] = v_acc[here, :].astype(BF)
        decay = jnp.sum(jnp.log(1.0 - gates(forget, slack_ref[...])), axis=0, keepdims=True)
        damping = jnp.sum(damp_ref[s], axis=1, keepdims=True)
        for h in range(heads):
            totals.append(decay[:, h * head_dim : (h + 1) * head_dim] + damping[h : h + 1, :])
    totals = jnp.concatenate(totals)
    for p in range(total_ref.shape[0]):
        total_ref[p] = totals


def log_totals(pieces, plan, weights, sums, slack, damp, parts):
    seqs, heads, _ = damp.shape
    return in_vmem(
        functools.partial(total_kernel, plan=plan),
        [jax.ShapeDtypeStruct(s.shape, BF) for s in sums]
        + [jax.ShapeDtypeStruct((parts, seqs * heads, weights[0].shape[1] // heads), F32)],
        *pieces,
        *weights,
        *sums,
        slack,
        damp,
        scratch=[pltpu.VMEM(s.shape, F32) for s in sums],
        flops=12 * len(pieces) * pieces[0].size * weights[0].shape[1],
    )


def state_kernel(forget_ref, value_ref, slack_ref, damp_ref, *refs):
    *outs, state_ref, parts_ref = refs
    far, rows, head_dim = parts_ref.shape[1], *parts_ref.shape[3:]
    seqs, heads, length = damp_ref.shape
    channels = heads * head_dim
    tall = length + 8
    row = lax.broadcasted_iota(jnp.int32, (tall, length), 0)
    column = lax.broadcasted_iota(jnp.int32, (tall, length), 1)
    later = jnp.where((column > row) | (row >= length), 1.0, 0.0).astype(BF)
    head = lax.broadcasted_iota(jnp.int32, (3 * heads, channels), 0) % heads
    channel = lax.broadcasted_iota(jnp.int32, (3 * heads, channels), 1)
    spread = jnp.where(channel // head_dim == head, 1.0, 0.0).astype(BF)
    over_rows = (((0,), (0,)), ((), ()))
    over_columns = (((1,), (1,)), ((), ()))
    totals = []
    for s in range(seqs):
        here = pl.ds(s * length, length)
        values = value_ref[here, :]
        gate = gates(forget_ref[here, :], slack_ref[...])
        high, middle, _ = three_terms(jnp.log(1.0 - gate))
        damping = lax.dot_general(
            later,
            jnp.concatenate(three_terms(damp_ref[s])),
            over_columns,
            preferred_element_type=F32,
        )
        damping = damping[:, :heads] + damping[:, heads : 2 * heads] + damping[:, 2 * heads :]
        sums = jnp.dot(
            jnp.concatenate([later, *three_terms(damping)], axis=1),
            jnp.concatenate([high, spread]),
            preferred_element_type=F32,
        ) + jnp.dot(later, middle, preferred_element_type=F32)
        weighted = (gate * jnp.exp(sums[:length])).astype(BF)
        for h in range(heads):
            cols = slice(h * head_dim, (h + 1) * head_dim)
            state = lax.dot_general(
                weighted[:, cols], values[:, cols], over_rows, preferred_element_type=F32
            )
            totals.append(sums[length : length + 1, cols])
            state = state.astype(BF)
            state_ref[s * heads + h] = state
            blocks = state.reshape(far, NEAR, rows, head_dim)
            for y in range(NEAR):
                parts_ref[y, :, s * heads + h] = blocks[:, y]
    pairs = seqs * heads
    terms = [t.astype(F32) for t in three_terms(jnp.concatenate(totals))]
    packed = jnp.concatenate([*terms, jnp.zeros((head_dim - 3 * pairs, head_dim), F32)])
    blocks = packed.T.astype(BF).reshape(far, NEAR, rows, head_dim)
    for y in range(NEAR):
        parts_ref[y, :, pairs] = blocks[:, y]
    near = lax.rem(lax.axis_index("sp"), NEAR)
    for step, out in enumerate(outs):
        out[...] = parts_ref[lax.rem(near + step, NEAR)]


def states(forget, values, slack, damp, parts):
    seqs, heads, _ = damp.shape
    head_dim = forget.shape[1] // heads
    pairs = seqs * heads
    shape = (parts // NEAR, pairs + 1, head_dim // parts, head_dim)
    *outs, state = in_vmem(
        state_kernel,
        [jax.ShapeDtypeStruct(shape, BF)] * NEAR
        + [jax.ShapeDtypeStruct((pairs, head_dim, head_dim), BF)],
        forget,
        values,
        slack,
        damp,
        scratch=[pltpu.VMEM((NEAR, *shape), BF)],
        flops=4 * forget.size * head_dim,
    )
    return outs, state


def unpacked(tile, pairs):
    tile = tile.astype(F32)
    lanes = tile.shape[1]
    return tile + pltpu.roll(tile, lanes - pairs, 1) + pltpu.roll(tile, lanes - 2 * pairs, 1)


def joined(tiles, place, count):
    pairs = tiles[0].shape[0] - 1
    places = [lax.rem(place + count - step, count) for step in range(count)]
    totals = [unpacked(tile[pairs], pairs) for tile in tiles]
    sums = [None] * pairs
    for here, tile in zip(places, tiles):
        after = sum(jnp.where(p > here, 1.0, 0.0) * total for p, total in zip(places, totals))
        scale = jnp.exp(after)
        for j in range(pairs):
            part = scale[:, j : j + 1] * tile[j].astype(F32)
            sums[j] = part if sums[j] is None else sums[j] + part
    return sums, sum(totals)


def near_kernel(*refs):
    tiles, outs, parts_ref = refs[:NEAR], refs[NEAR:-1], refs[-1]
    far, tile_count, rows, lanes = parts_ref.shape
    pairs = tile_count - 1
    me = lax.axis_index("sp")
    lane = lax.broadcasted_iota(jnp.int32, (rows, lanes), 1)
    for z in range(far):
        sums, total = joined([t.at[z] for t in tiles], lax.rem(me, NEAR), NEAR)
        for j in range(pairs):
            parts_ref[z, j] = sums[j].astype(BF)
        high, middle, low = (t.astype(F32) for t in three_terms(total))
        packed = jnp.where(lane < 2 * pairs, pltpu.roll(middle, pairs, 1), pltpu.roll(low, 2 * pairs, 1))
        packed = jnp.where(lane < pairs, high, packed)
        parts_ref[z, pairs] = jnp.where(lane < 3 * pairs, packed, 0.0).astype(BF)
    for step, out in enumerate(outs):
        out[...] = parts_ref[lax.rem(me // NEAR + step, far)]


def join_near(tiles):
    shape = tiles[0].shape
    return in_vmem(
        near_kernel,
        [jax.ShapeDtypeStruct(shape[1:], BF)] * shape[0],
        *tiles,
        scratch=[pltpu.VMEM(shape, BF)],
    )


def far_kernel(*refs):
    tiles, cache_ref = refs[:-1], refs[-1]
    sums, _ = joined(tiles, lax.axis_index("sp") // NEAR, len(tiles))
    for j, part in enumerate(sums):
        cache_ref[j] = part.astype(BF)


def join_far(tiles):
    tile_count, rows, lanes = tiles[0].shape
    return in_vmem(far_kernel, pltpu.VMEM((tile_count - 1, rows, lanes), BF), *tiles)


def read_kernel(totals_ref, state_ref, query_ref, keys_ref, out_ref):
    me = lax.axis_index("sp")
    after = sum(
        jnp.where(src > me, 1.0, 0.0) * totals_ref[src] for src in range(totals_ref.shape[0])
    )
    weights = query_ref[...] * (1.0 - keys_ref[...]) * jnp.exp(after)
    pairs = weights.shape[0]
    terms = jnp.concatenate(three_terms(weights))
    reads = []
    for j in range(pairs):
        parts = jnp.dot(terms, state_ref[j], preferred_element_type=F32)
        reads.append(sum(parts[n : n + 1, :] for n in range(j, 3 * pairs, pairs)))
    reads = jnp.concatenate(reads)
    for p in range(out_ref.shape[0]):
        out_ref[p] = reads


def read_parts(totals, state, query, keys):
    return in_vmem(read_kernel, jax.ShapeDtypeStruct(totals.shape, F32), totals, state, query, keys)


def finish_kernel(got_ref, query_ref, keys_ref, value_ref, norm_ref, gate_ref, out_ref):
    heads = out_ref.shape[1] // got_ref.shape[2]
    head_dim = got_ref.shape[2]
    shared = jnp.sum(query_ref[...] * keys_ref[...], axis=1, keepdims=True)
    read = shared * value_ref[...]
    for src in range(got_ref.shape[0]):
        read = read + got_ref[src]
    scaled = read * lax.rsqrt(jnp.mean(read * read, axis=1, keepdims=True) + 1e-06) * norm_ref[...]
    result = (scaled * gate_ref[...]).astype(BF)
    for s in range(out_ref.shape[0]):
        for h in range(heads):
            j = s * heads + h
            out_ref[s : s + 1, h * head_dim : (h + 1) * head_dim] = result[j : j + 1, :]


def new_token_kernel(x_ref, q_hbm, g_hbm, f_hbm, v_hbm, out_ref, x_here, rows, sems):
    seqs, slab = x_ref.shape
    here = pl.ds(pl.multiple_of(lax.axis_index("sp") * slab, slab), slab)
    sources = (q_hbm, g_hbm, f_hbm.at[here], v_hbm.at[here])
    copied([(w, rows.at[n]) for n, w in enumerate(sources)] + [(x_ref, x_here)], sems)
    for n in range(len(sources)):
        y = jnp.dot(x_here[...], rows[n], preferred_element_type=F32)
        for p in range(out_ref.shape[0]):
            out_ref[p, n * seqs : (n + 1) * seqs, :] = y


def prepare_kernel(got_ref, slack_ref, query_ref, keys_ref, value_ref, gate_ref):
    pairs, head_dim = value_ref.shape
    seqs = got_ref.shape[1] // 4
    heads = pairs // seqs
    total = got_ref[0]
    for src in range(1, got_ref.shape[0]):
        total = total + got_ref[src]
    rounded = total.astype(BF).astype(F32)

    def by_head(x):
        return jnp.concatenate(
            [
                x[s : s + 1, h * head_dim : (h + 1) * head_dim]
                for s in range(x.shape[0])
                for h in range(heads)
            ]
        )

    query, gate, forget, value = (rounded[n * seqs : (n + 1) * seqs] for n in range(4))
    keys = slack_ref[...] * jax.nn.sigmoid(-forget)
    value_ref[...] = by_head(value)
    gate_ref[...] = by_head(gate * jax.nn.sigmoid(gate))
    query_ref[...] = by_head(query)
    keys_ref[...] = by_head(keys)


def per_device(
    tokens,
    first_token_input,
    forget_weight,
    value_weight,
    query_weight,
    output_gate_weight,
    forget_bound_slack,
    additional_damping_exponent,
    read_norm_scale,
):
    seqs, length, width = tokens.shape
    head_dim = read_norm_scale.shape[0]
    heads = additional_damping_exponent.shape[2]
    channels = heads * head_dim
    sp_count = lax.axis_size("sp")
    tp_count = lax.axis_size("tp")
    chips = tp_count // 2
    slack = forget_bound_slack.reshape(1, channels)

    def shifted(x, by):
        pairs = [(2 * c + k, 2 * ((c + by) % chips) + k) for c in range(chips) for k in (0, 1)]
        return lax.ppermute(x, "tp", pairs)

    def sibling(x):
        return lax.ppermute(x, "tp", [(i, i ^ 1) for i in range(tp_count)])

    def exchange(x):
        return lax.all_to_all(x, "sp", 0, 0, tiled=True)

    rows = seqs // 2 * length
    own_a, own_b = (x.reshape(rows, width) for x in split(tokens, 2))
    right_a, left_a = shifted(own_a, 1), shifted(own_a, -1)
    right_b, left_b = shifted(own_b, 1), shifted(own_b, -1)
    other_a, other_b = sibling(own_a), sibling(own_b)

    partial = in_vmem(
        new_token_kernel,
        jax.ShapeDtypeStruct((sp_count, 4 * seqs, channels), F32),
        *(
            pltpu.with_memory_space_constraint(x, pltpu.HBM)
            for x in (
                first_token_input,
                query_weight,
                output_gate_weight,
                forget_weight,
                value_weight,
            )
        ),
        in_specs=[pl.BlockSpec(memory_space=pltpu.HBM)] * 5,
        scratch=[
            pltpu.VMEM(first_token_input.shape, BF),
            pltpu.VMEM((4, *query_weight.shape), BF),
            pltpu.SemaphoreType.DMA((5,)),
        ],
    )
    new_sums = exchange(partial)
    row_count = head_dim // sp_count
    pairs = seqs * heads
    query_new, keys_new, value_new, gate_new = in_vmem(
        prepare_kernel, [jax.ShapeDtypeStruct((pairs, head_dim), F32)] * 4, new_sums, slack
    )

    far_a, far_b = shifted(right_a, 1), shifted(left_b, -1)
    other_right_a, other_left_a = sibling(right_a), sibling(left_a)
    other_right_b, other_left_b = sibling(right_b), sibling(left_b)
    other_far_a, other_far_b = sibling(far_a), sibling(far_b)

    def both(by):
        return ((by, False), (by, True))

    weights, sums = load_and_project(
        [own_a, other_a, own_b, other_b], (both(0), both(0)), (forget_weight, value_weight)
    )
    pieces = [right_a, other_right_a, left_b, other_left_b]
    sums = project(pieces, (both(1), both(-1)), weights, sums)
    pieces = [left_a, other_left_a, right_b, other_right_b]
    sums = project(pieces, (both(-1), both(1)), weights, sums)
    damp = additional_damping_exponent.transpose(0, 2, 1)
    forget, values, totals = log_totals(
        [far_a, other_far_a, far_b, other_far_b],
        (both(2), both(2)),
        weights,
        sums,
        slack,
        damp,
        sp_count,
    )
    parts, state = states(forget, values, slack, damp, sp_count)

    planes = sp_count // NEAR

    def along_y(step):
        pairs = [
            (z * NEAR + y, z * NEAR + (y + step) % NEAR) for z in range(planes) for y in range(NEAR)
        ]
        return lax.ppermute(parts[step], "sp", pairs)

    def along_z(step):
        pairs = [
            (z * NEAR + y, (z + step) % planes * NEAR + y)
            for z in range(planes)
            for y in range(NEAR)
        ]
        return lax.ppermute(parts[step], "sp", pairs)

    parts = [parts[0], *(along_y(step) for step in range(1, NEAR))]
    parts = join_near(parts)
    parts = [parts[0], *(along_z(step) for step in range(1, planes))]
    cache = join_far(parts)

    totals = exchange(totals)
    read = read_parts(totals, state, query_new, keys_new)
    got = exchange(read)
    first_read = in_vmem(
        finish_kernel,
        jax.ShapeDtypeStruct((seqs, channels), BF),
        got,
        query_new,
        keys_new,
        value_new,
        read_norm_scale.reshape(1, head_dim),
        gate_new,
    )
    return cache.reshape(seqs, heads, row_count, head_dim), first_read


def solution(mesh):
    placed = (
        P("gr", "sp", "tp"),
        P("gr", "sp"),
        P(None, "tp"),
        P(None, "tp"),
        P("sp", "tp"),
        P("sp", "tp"),
        P("tp"),
        P("gr", "sp", "tp"),
        P(),
    )

    return jax.shard_map(
        per_device,
        mesh=mesh,
        in_specs=placed,
        out_specs=(P("gr", "tp", "sp", None), P("gr", "tp")),
        check_vma=False,
    )
```

```python
import functools

import jax
import jax.numpy as jnp
from jax import lax
from jax.experimental import pallas as pl
from jax.experimental.pallas import tpu as pltpu
from jax.sharding import PartitionSpec as P


BF = jnp.bfloat16
F32 = jnp.float32
NEAR = 4


def three_terms(x):
    high = x.astype(BF)
    rest = x - high.astype(F32)
    middle = rest.astype(BF)
    low = (rest - middle.astype(F32)).astype(BF)
    return high, middle, low


VMEM = pl.BlockSpec(memory_space=pltpu.VMEM)


def in_vmem(kernel, out_shape, *arrays, in_specs=None, scratch=(), flops=0):
    return pl.pallas_call(
        kernel,
        in_specs=in_specs or [VMEM] * len(arrays),
        out_specs=jax.tree.map(lambda _: VMEM, out_shape),
        out_shape=out_shape,
        scratch_shapes=scratch,
        compiler_params=pltpu.CompilerParams(vmem_limit_bytes=12 << 20),
        cost_estimate=pl.CostEstimate(flops=flops, transcendentals=0, bytes_accessed=0),
    )(*arrays)


def copied(pairs, sems):
    copies = [pltpu.make_async_copy(*pair, sems.at[n]) for n, pair in enumerate(pairs)]
    for copy in copies:
        copy.start()
    for copy in copies:
        copy.wait()


def from_hbm(kernel, shapes, *arrays):
    return pl.pallas_call(
        kernel,
        in_specs=[pl.BlockSpec(memory_space=pltpu.HBM)] * len(arrays),
        out_specs=[VMEM] * len(shapes),
        out_shape=[pltpu.VMEM(shape, BF) for shape in shapes],
        scratch_shapes=[pltpu.SemaphoreType.DMA((len(shapes),))],
        compiler_params=pltpu.CompilerParams(vmem_limit_bytes=1 << 20),
    )(*(pltpu.with_memory_space_constraint(a, pltpu.HBM) for a in arrays))


def split_kernel(tokens_ref, *refs):
    seqs = tokens_ref.shape[0] // (len(refs) - 1)
    copied(
        [(tokens_ref.at[pl.ds(n * seqs, seqs)], out) for n, out in enumerate(refs[:-1])], refs[-1]
    )


def split(tokens, count):
    shape = (tokens.shape[0] // count, *tokens.shape[1:])
    return from_hbm(split_kernel, [shape] * count, tokens)


def block_of(tp, by, other):
    count = lax.axis_size("tp")
    return lax.rem((tp ^ 1 if other else tp) + count - 2 * by, count)


def products(pieces, sources, w_ref):
    tp = lax.axis_index("tp")
    total = None
    for piece, source in zip(pieces, sources):
        width = piece.shape[1]
        start = pl.multiple_of(block_of(tp, *source) * width, width)
        part = jnp.dot(piece[...], w_ref[pl.ds(start, width), :], preferred_element_type=F32)
        total = part if total is None else total + part
    return total


def add_products(pieces, plan, weights, sums, outs):
    rows = pieces[0].shape[0]
    for half, sources in enumerate(plan):
        here = pl.ds(half * rows, rows)
        some, pieces = pieces[: len(sources)], pieces[len(sources) :]
        for n, (w_ref, out) in enumerate(zip(weights, outs)):
            result = products(some, sources, w_ref)
            out[here, :] = sums[n][here, :] + result if sums else result


def project_kernel(*refs, plan):
    count = sum(map(len, plan))
    add_products(refs[:count], plan, refs[count : count + 2], refs[-4:-2], refs[-2:])


def project(pieces, plan, weights, sums):
    return in_vmem(
        functools.partial(project_kernel, plan=plan),
        [jax.ShapeDtypeStruct(s.shape, F32) for s in sums],
        *pieces,
        *weights,
        *sums,
        flops=4 * len(pieces) * pieces[0].size * weights[0].shape[1],
    )


def load_kernel(own_hbm, other_hbm, wf_hbm, wv_hbm, *refs, plan):
    wf_ref, wv_ref, *outs, own_ref, other_ref, sems = refs
    chips = lax.axis_size("tp") // 2
    depth = wf_ref.shape[0] // chips
    chip = lax.axis_index("tp") // 2
    pairs = [(own_hbm, own_ref), (other_hbm, other_ref)]
    for step in range(chips):
        here = pl.ds(pl.multiple_of(lax.rem(chip + step, chips) * depth, depth), depth)
        pairs += [(wf_hbm.at[here], wf_ref.at[here]), (wv_hbm.at[here], wv_ref.at[here])]
    copies = [pltpu.make_async_copy(*pair, sems.at[n]) for n, pair in enumerate(pairs)]
    for copy in copies:
        copy.start()
    for copy in copies[:4]:
        copy.wait()
    add_products((own_ref, other_ref), plan, (wf_ref, wv_ref), (), outs)
    for copy in copies[4:]:
        copy.wait()


def load_and_project(own, other, plan, weights):
    out = jax.ShapeDtypeStruct((own.shape[0], weights[0].shape[1]), F32)
    *weights, f, v = pl.pallas_call(
        functools.partial(load_kernel, plan=plan),
        in_specs=[pl.BlockSpec(memory_space=pltpu.HBM)] * 4,
        out_specs=[VMEM] * 4,
        out_shape=[pltpu.VMEM(w.shape, BF) for w in weights] + [out] * 2,
        scratch_shapes=[pltpu.VMEM(own.shape, BF)] * 2
        + [pltpu.SemaphoreType.DMA((lax.axis_size("tp") + 2,))],
        compiler_params=pltpu.CompilerParams(vmem_limit_bytes=12 << 20),
        name="load",
    )(*(pltpu.with_memory_space_constraint(x, pltpu.HBM) for x in (own, other, *weights)))
    return [pltpu.with_memory_space_constraint(w, pltpu.VMEM) for w in weights], [f, v]


def gates(forget, slack):
    return slack / (1.0 + jnp.exp(forget.astype(F32)))


def total_kernel(*refs, plan):
    count = sum(map(len, plan))
    pieces, (wf_ref, wv_ref, f_in, v_in, *refs) = refs[:count], refs[count:]
    slack_ref, damp_ref, f_out, v_out, total_ref, f_acc, v_acc = refs
    add_products(pieces, plan, (wf_ref, wv_ref), (f_in, v_in), (f_acc, v_acc))
    seqs, heads, length = damp_ref.shape
    head_dim = total_ref.shape[2]
    totals = []
    for s in range(seqs):
        here = pl.ds(s * length, length)
        forget = f_acc[here, :].astype(BF)
        f_out[here, :] = forget
        v_out[here, :] = v_acc[here, :].astype(BF)
        decay = jnp.sum(jnp.log(1.0 - gates(forget, slack_ref[...])), axis=0, keepdims=True)
        damping = jnp.sum(damp_ref[s], axis=1, keepdims=True)
        for h in range(heads):
            totals.append(decay[:, h * head_dim : (h + 1) * head_dim] + damping[h : h + 1, :])
    totals = jnp.concatenate(totals)
    for p in range(total_ref.shape[0]):
        total_ref[p] = totals


def log_totals(pieces, plan, weights, sums, slack, damp, parts):
    seqs, heads, _ = damp.shape
    return in_vmem(
        functools.partial(total_kernel, plan=plan),
        [jax.ShapeDtypeStruct(s.shape, BF) for s in sums]
        + [jax.ShapeDtypeStruct((parts, seqs * heads, weights[0].shape[1] // heads), F32)],
        *pieces,
        *weights,
        *sums,
        slack,
        damp,
        scratch=[pltpu.VMEM(s.shape, F32) for s in sums],
        flops=12 * len(pieces) * pieces[0].size * weights[0].shape[1],
    )


def state_kernel(forget_ref, value_ref, slack_ref, damp_ref, *refs):
    *outs, state_ref, parts_ref = refs
    far, rows, head_dim = parts_ref.shape[1], *parts_ref.shape[3:]
    seqs, heads, length = damp_ref.shape
    channels = heads * head_dim
    tall = length + 8
    row = lax.broadcasted_iota(jnp.int32, (tall, length), 0)
    column = lax.broadcasted_iota(jnp.int32, (tall, length), 1)
    later = jnp.where((column > row) | (row >= length), 1.0, 0.0).astype(BF)
    head = lax.broadcasted_iota(jnp.int32, (3 * heads, channels), 0) % heads
    channel = lax.broadcasted_iota(jnp.int32, (3 * heads, channels), 1)
    spread = jnp.where(channel // head_dim == head, 1.0, 0.0).astype(BF)
    over_rows = (((0,), (0,)), ((), ()))
    over_columns = (((1,), (1,)), ((), ()))
    totals = []
    for s in range(seqs):
        here = pl.ds(s * length, length)
        values = value_ref[here, :]
        gate = gates(forget_ref[here, :], slack_ref[...])
        high, middle, _ = three_terms(jnp.log(1.0 - gate))
        damping = lax.dot_general(
            later,
            jnp.concatenate(three_terms(damp_ref[s])),
            over_columns,
            preferred_element_type=F32,
        )
        damping = damping[:, :heads] + damping[:, heads : 2 * heads] + damping[:, 2 * heads :]
        sums = jnp.dot(
            jnp.concatenate([later, *three_terms(damping)], axis=1),
            jnp.concatenate([high, spread]),
            preferred_element_type=F32,
        ) + jnp.dot(later, middle, preferred_element_type=F32)
        weighted = (gate * jnp.exp(sums[:length])).astype(BF)
        for h in range(heads):
            cols = slice(h * head_dim, (h + 1) * head_dim)
            state = lax.dot_general(
                weighted[:, cols], values[:, cols], over_rows, preferred_element_type=F32
            )
            totals.append(sums[length : length + 1, cols])
            state = state.astype(BF)
            state_ref[s * heads + h] = state
            blocks = state.reshape(far, NEAR, rows, head_dim)
            for y in range(NEAR):
                parts_ref[y, :, s * heads + h] = blocks[:, y]
    pairs = seqs * heads
    terms = [t.astype(F32) for t in three_terms(jnp.concatenate(totals))]
    packed = jnp.concatenate([*terms, jnp.zeros((head_dim - 3 * pairs, head_dim), F32)])
    blocks = packed.T.astype(BF).reshape(far, NEAR, rows, head_dim)
    for y in range(NEAR):
        parts_ref[y, :, pairs] = blocks[:, y]
    near = lax.rem(lax.axis_index("sp"), NEAR)
    for step, out in enumerate(outs):
        out[...] = parts_ref[lax.rem(near + step, NEAR)]


def states(forget, values, slack, damp, parts):
    seqs, heads, _ = damp.shape
    head_dim = forget.shape[1] // heads
    pairs = seqs * heads
    shape = (parts // NEAR, pairs + 1, head_dim // parts, head_dim)
    *outs, state = in_vmem(
        state_kernel,
        [jax.ShapeDtypeStruct(shape, BF)] * NEAR
        + [jax.ShapeDtypeStruct((pairs, head_dim, head_dim), BF)],
        forget,
        values,
        slack,
        damp,
        scratch=[pltpu.VMEM((NEAR, *shape), BF)],
        flops=4 * forget.size * head_dim,
    )
    return outs, state


def unpacked(tile, pairs):
    tile = tile.astype(F32)
    lanes = tile.shape[1]
    return tile + pltpu.roll(tile, lanes - pairs, 1) + pltpu.roll(tile, lanes - 2 * pairs, 1)


def joined(tiles, place, count):
    pairs = tiles[0].shape[0] - 1
    places = [lax.rem(place + count - step, count) for step in range(count)]
    totals = [unpacked(tile[pairs], pairs) for tile in tiles]
    sums = [None] * pairs
    for here, tile in zip(places, tiles):
        after = sum(jnp.where(p > here, 1.0, 0.0) * total for p, total in zip(places, totals))
        scale = jnp.exp(after)
        for j in range(pairs):
            part = scale[:, j : j + 1] * tile[j].astype(F32)
            sums[j] = part if sums[j] is None else sums[j] + part
    return sums, sum(totals)


def near_kernel(*refs):
    tiles, outs, parts_ref = refs[:NEAR], refs[NEAR:-1], refs[-1]
    far, tile_count, rows, lanes = parts_ref.shape
    pairs = tile_count - 1
    me = lax.axis_index("sp")
    lane = lax.broadcasted_iota(jnp.int32, (rows, lanes), 1)
    for z in range(far):
        sums, total = joined([t.at[z] for t in tiles], lax.rem(me, NEAR), NEAR)
        for j in range(pairs):
            parts_ref[z, j] = sums[j].astype(BF)
        high, middle, low = (t.astype(F32) for t in three_terms(total))
        packed = jnp.where(lane < 2 * pairs, pltpu.roll(middle, pairs, 1), pltpu.roll(low, 2 * pairs, 1))
        packed = jnp.where(lane < pairs, high, packed)
        parts_ref[z, pairs] = jnp.where(lane < 3 * pairs, packed, 0.0).astype(BF)
    for step, out in enumerate(outs):
        out[...] = parts_ref[lax.rem(me // NEAR + step, far)]


def join_near(tiles):
    shape = tiles[0].shape
    return in_vmem(
        near_kernel,
        [jax.ShapeDtypeStruct(shape[1:], BF)] * shape[0],
        *tiles,
        scratch=[pltpu.VMEM(shape, BF)],
    )


def far_kernel(*refs):
    tiles, cache_ref = refs[:-1], refs[-1]
    sums, _ = joined(tiles, lax.axis_index("sp") // NEAR, len(tiles))
    for j, part in enumerate(sums):
        cache_ref[j] = part.astype(BF)


def join_far(tiles):
    tile_count, rows, lanes = tiles[0].shape
    return in_vmem(far_kernel, pltpu.VMEM((tile_count - 1, rows, lanes), BF), *tiles)


def read_kernel(totals_ref, state_ref, query_ref, keys_ref, out_ref):
    me = lax.axis_index("sp")
    after = sum(
        jnp.where(src > me, 1.0, 0.0) * totals_ref[src] for src in range(totals_ref.shape[0])
    )
    weights = query_ref[...] * (1.0 - keys_ref[...]) * jnp.exp(after)
    pairs = weights.shape[0]
    terms = jnp.concatenate(three_terms(weights))
    reads = []
    for j in range(pairs):
        parts = jnp.dot(terms, state_ref[j], preferred_element_type=F32)
        reads.append(sum(parts[n : n + 1, :] for n in range(j, 3 * pairs, pairs)))
    reads = jnp.concatenate(reads)
    for p in range(out_ref.shape[0]):
        out_ref[p] = reads


def read_parts(totals, state, query, keys):
    return in_vmem(read_kernel, jax.ShapeDtypeStruct(totals.shape, F32), totals, state, query, keys)


def finish_kernel(got_ref, query_ref, keys_ref, value_ref, norm_ref, gate_ref, out_ref):
    heads = out_ref.shape[1] // got_ref.shape[2]
    head_dim = got_ref.shape[2]
    shared = jnp.sum(query_ref[...] * keys_ref[...], axis=1, keepdims=True)
    read = shared * value_ref[...]
    for src in range(got_ref.shape[0]):
        read = read + got_ref[src]
    scaled = read * lax.rsqrt(jnp.mean(read * read, axis=1, keepdims=True) + 1e-06) * norm_ref[...]
    result = (scaled * gate_ref[...]).astype(BF)
    for s in range(out_ref.shape[0]):
        for h in range(heads):
            j = s * heads + h
            out_ref[s : s + 1, h * head_dim : (h + 1) * head_dim] = result[j : j + 1, :]


def new_token_kernel(x_ref, q_hbm, g_hbm, f_hbm, v_hbm, out_ref, x_here, rows, sems):
    seqs, slab = x_ref.shape
    here = pl.ds(pl.multiple_of(lax.axis_index("sp") * slab, slab), slab)
    sources = (q_hbm, g_hbm, f_hbm.at[here], v_hbm.at[here])
    copied([(w, rows.at[n]) for n, w in enumerate(sources)] + [(x_ref, x_here)], sems)
    for n in range(len(sources)):
        y = jnp.dot(x_here[...], rows[n], preferred_element_type=F32)
        for p in range(out_ref.shape[0]):
            out_ref[p, n * seqs : (n + 1) * seqs, :] = y


def prepare_kernel(got_ref, slack_ref, query_ref, keys_ref, value_ref, gate_ref):
    pairs, head_dim = value_ref.shape
    seqs = got_ref.shape[1] // 4
    heads = pairs // seqs
    total = got_ref[0]
    for src in range(1, got_ref.shape[0]):
        total = total + got_ref[src]
    rounded = total.astype(BF).astype(F32)

    def by_head(x):
        return jnp.concatenate(
            [
                x[s : s + 1, h * head_dim : (h + 1) * head_dim]
                for s in range(x.shape[0])
                for h in range(heads)
            ]
        )

    query, gate, forget, value = (rounded[n * seqs : (n + 1) * seqs] for n in range(4))
    keys = slack_ref[...] * jax.nn.sigmoid(-forget)
    value_ref[...] = by_head(value)
    gate_ref[...] = by_head(gate * jax.nn.sigmoid(gate))
    query_ref[...] = by_head(query)
    keys_ref[...] = by_head(keys)


def per_device(
    tokens,
    first_token_input,
    forget_weight,
    value_weight,
    query_weight,
    output_gate_weight,
    forget_bound_slack,
    additional_damping_exponent,
    read_norm_scale,
):
    seqs, length, width = tokens.shape
    head_dim = read_norm_scale.shape[0]
    heads = additional_damping_exponent.shape[2]
    channels = heads * head_dim
    sp_count = lax.axis_size("sp")
    tp_count = lax.axis_size("tp")
    chips = tp_count // 2
    slack = forget_bound_slack.reshape(1, channels)

    def shifted(x, by):
        pairs = [(2 * c + k, 2 * ((c + by) % chips) + k) for c in range(chips) for k in (0, 1)]
        return lax.ppermute(x, "tp", pairs)

    def sibling(x):
        return lax.ppermute(x, "tp", [(i, i ^ 1) for i in range(tp_count)])

    def exchange(x):
        return lax.all_to_all(x, "sp", 0, 0, tiled=True)

    rows = seqs // 2 * length
    own = tokens.reshape(seqs * length, width)
    other = sibling(own)
    own_a, own_b = (x.reshape(rows, width) for x in split(tokens, 2))
    right_a, left_a = shifted(own_a, 1), shifted(own_a, -1)
    right_b, left_b = shifted(own_b, 1), shifted(own_b, -1)

    partial = in_vmem(
        new_token_kernel,
        jax.ShapeDtypeStruct((sp_count, 4 * seqs, channels), F32),
        *(
            pltpu.with_memory_space_constraint(x, pltpu.HBM)
            for x in (
                first_token_input,
                query_weight,
                output_gate_weight,
                forget_weight,
                value_weight,
            )
        ),
        in_specs=[pl.BlockSpec(memory_space=pltpu.HBM)] * 5,
        scratch=[
            pltpu.VMEM(first_token_input.shape, BF),
            pltpu.VMEM((4, *query_weight.shape), BF),
            pltpu.SemaphoreType.DMA((5,)),
        ],
    )
    new_sums = exchange(partial)
    row_count = head_dim // sp_count
    pairs = seqs * heads
    query_new, keys_new, value_new, gate_new = in_vmem(
        prepare_kernel, [jax.ShapeDtypeStruct((pairs, head_dim), F32)] * 4, new_sums, slack
    )

    far_a, far_b = shifted(right_a, 1), shifted(left_b, -1)
    other_right_a, other_left_a = sibling(right_a), sibling(left_a)
    other_right_b, other_left_b = sibling(right_b), sibling(left_b)
    other_far_a, other_far_b = sibling(far_a), sibling(far_b)

    def both(by):
        return ((by, False), (by, True))

    weights, sums = load_and_project(
        own, other, (both(0),), (forget_weight, value_weight)
    )
    pieces = [right_a, other_right_a, left_b, other_left_b]
    sums = project(pieces, (both(1), both(-1)), weights, sums)
    pieces = [left_a, other_left_a, right_b, other_right_b]
    sums = project(pieces, (both(-1), both(1)), weights, sums)
    damp = additional_damping_exponent.transpose(0, 2, 1)
    forget, values, totals = log_totals(
        [far_a, other_far_a, far_b, other_far_b],
        (both(2), both(2)),
        weights,
        sums,
        slack,
        damp,
        sp_count,
    )
    parts, state = states(forget, values, slack, damp, sp_count)

    planes = sp_count // NEAR

    def along_y(step):
        pairs = [
            (z * NEAR + y, z * NEAR + (y + step) % NEAR) for z in range(planes) for y in range(NEAR)
        ]
        return lax.ppermute(parts[step], "sp", pairs)

    def along_z(step):
        pairs = [
            (z * NEAR + y, (z + step) % planes * NEAR + y)
            for z in range(planes)
            for y in range(NEAR)
        ]
        return lax.ppermute(parts[step], "sp", pairs)

    parts = [parts[0], *(along_y(step) for step in range(1, NEAR))]
    parts = join_near(parts)
    parts = [parts[0], *(along_z(step) for step in range(1, planes))]
    cache = join_far(parts)

    totals = exchange(totals)
    read = read_parts(totals, state, query_new, keys_new)
    got = exchange(read)
    first_read = in_vmem(
        finish_kernel,
        jax.ShapeDtypeStruct((seqs, channels), BF),
        got,
        query_new,
        keys_new,
        value_new,
        read_norm_scale.reshape(1, head_dim),
        gate_new,
    )
    return cache.reshape(seqs, heads, row_count, head_dim), first_read


def solution(mesh):
    placed = (
        P("gr", "sp", "tp"),
        P("gr", "sp"),
        P(None, "tp"),
        P(None, "tp"),
        P("sp", "tp"),
        P("sp", "tp"),
        P("tp"),
        P("gr", "sp", "tp"),
        P(),
    )

    return jax.shard_map(
        per_device,
        mesh=mesh,
        in_specs=placed,
        out_specs=(P("gr", "tp", "sp", None), P("gr", "tp")),
        check_vma=False,
    )
```

```python
import functools

import jax
import jax.numpy as jnp
from jax import lax
from jax.experimental import pallas as pl
from jax.experimental.pallas import tpu as pltpu
from jax.sharding import PartitionSpec as P


BF = jnp.bfloat16
F32 = jnp.float32
NEAR = 4


def three_terms(x):
    high = x.astype(BF)
    rest = x - high.astype(F32)
    middle = rest.astype(BF)
    low = (rest - middle.astype(F32)).astype(BF)
    return high, middle, low


VMEM = pl.BlockSpec(memory_space=pltpu.VMEM)


def in_vmem(kernel, out_shape, *arrays, in_specs=None, scratch=(), flops=0):
    return pl.pallas_call(
        kernel,
        in_specs=in_specs or [VMEM] * len(arrays),
        out_specs=jax.tree.map(lambda _: VMEM, out_shape),
        out_shape=out_shape,
        scratch_shapes=scratch,
        compiler_params=pltpu.CompilerParams(vmem_limit_bytes=12 << 20),
        cost_estimate=pl.CostEstimate(flops=flops, transcendentals=0, bytes_accessed=0),
    )(*arrays)


def copied(pairs, sems):
    copies = [pltpu.make_async_copy(*pair, sems.at[n]) for n, pair in enumerate(pairs)]
    for copy in copies:
        copy.start()
    for copy in copies:
        copy.wait()


def from_hbm(kernel, shapes, *arrays):
    return pl.pallas_call(
        kernel,
        in_specs=[pl.BlockSpec(memory_space=pltpu.HBM)] * len(arrays),
        out_specs=[VMEM] * len(shapes),
        out_shape=[pltpu.VMEM(shape, BF) for shape in shapes],
        scratch_shapes=[pltpu.SemaphoreType.DMA((len(shapes),))],
        compiler_params=pltpu.CompilerParams(vmem_limit_bytes=1 << 20),
    )(*(pltpu.with_memory_space_constraint(a, pltpu.HBM) for a in arrays))


def split_kernel(tokens_ref, *refs):
    seqs = tokens_ref.shape[0] // (len(refs) - 1)
    copied(
        [(tokens_ref.at[pl.ds(n * seqs, seqs)], out) for n, out in enumerate(refs[:-1])], refs[-1]
    )


def split(tokens, count):
    shape = (tokens.shape[0] // count, *tokens.shape[1:])
    return from_hbm(split_kernel, [shape] * count, tokens)


def block_of(tp, by, other):
    count = lax.axis_size("tp")
    return lax.rem((tp ^ 1 if other else tp) + count - 2 * by, count)


def products(pieces, sources, w_ref):
    tp = lax.axis_index("tp")
    total = None
    for piece, source in zip(pieces, sources):
        width = piece.shape[1]
        start = pl.multiple_of(block_of(tp, *source) * width, width)
        part = jnp.dot(piece[...], w_ref[pl.ds(start, width), :], preferred_element_type=F32)
        total = part if total is None else total + part
    return total


def add_products(pieces, plan, weights, sums, outs):
    rows = pieces[0].shape[0]
    for half, sources in enumerate(plan):
        here = pl.ds(half * rows, rows)
        some, pieces = pieces[: len(sources)], pieces[len(sources) :]
        for n, (w_ref, out) in enumerate(zip(weights, outs)):
            result = products(some, sources, w_ref)
            out[here, :] = sums[n][here, :] + result if sums else result


def project_kernel(*refs, plan):
    count = sum(map(len, plan))
    add_products(refs[:count], plan, refs[count : count + 2], refs[-4:-2], refs[-2:])


def project(pieces, plan, weights, sums):
    return in_vmem(
        functools.partial(project_kernel, plan=plan),
        [jax.ShapeDtypeStruct(s.shape, F32) for s in sums],
        *pieces,
        *weights,
        *sums,
        flops=4 * len(pieces) * pieces[0].size * weights[0].shape[1],
    )


def load_kernel(own_hbm, other_hbm, wf_hbm, wv_hbm, *refs, plan):
    wf_ref, wv_ref, *outs, own_ref, other_ref, sems = refs
    chips = lax.axis_size("tp") // 2
    depth = wf_ref.shape[0] // chips
    chip = lax.axis_index("tp") // 2
    pairs = [(own_hbm, own_ref), (other_hbm, other_ref)]
    for step in range(chips):
        here = pl.ds(pl.multiple_of(lax.rem(chip + step, chips) * depth, depth), depth)
        pairs += [(wf_hbm.at[here], wf_ref.at[here]), (wv_hbm.at[here], wv_ref.at[here])]
    copies = [pltpu.make_async_copy(*pair, sems.at[n]) for n, pair in enumerate(pairs)]
    for copy in copies:
        copy.start()
    for copy in copies[:4]:
        copy.wait()
    add_products((own_ref, other_ref), plan, (wf_ref, wv_ref), (), outs)
    for copy in copies[4:]:
        copy.wait()


def load_and_project(own, other, plan, weights):
    out = jax.ShapeDtypeStruct((own.shape[0], weights[0].shape[1]), F32)
    *weights, f, v = pl.pallas_call(
        functools.partial(load_kernel, plan=plan),
        in_specs=[pl.BlockSpec(memory_space=pltpu.HBM)] * 4,
        out_specs=[VMEM] * 4,
        out_shape=[pltpu.VMEM(w.shape, BF) for w in weights] + [out] * 2,
        scratch_shapes=[pltpu.VMEM(own.shape, BF)] * 2
        + [pltpu.SemaphoreType.DMA((lax.axis_size("tp") + 2,))],
        compiler_params=pltpu.CompilerParams(vmem_limit_bytes=12 << 20),
        name="load",
    )(*(pltpu.with_memory_space_constraint(x, pltpu.HBM) for x in (own, other, *weights)))
    return [pltpu.with_memory_space_constraint(w, pltpu.VMEM) for w in weights], [f, v]


def gates(forget, slack):
    return slack / (1.0 + jnp.exp(forget.astype(F32)))


def total_kernel(*refs, plan):
    count = sum(map(len, plan))
    pieces, (wf_ref, wv_ref, f_in, v_in, *refs) = refs[:count], refs[count:]
    slack_ref, damp_ref, f_out, v_out, total_ref, f_acc, v_acc = refs
    add_products(pieces, plan, (wf_ref, wv_ref), (f_in, v_in), (f_acc, v_acc))
    seqs, heads, length = damp_ref.shape
    head_dim = total_ref.shape[2]
    totals = []
    for s in range(seqs):
        here = pl.ds(s * length, length)
        forget = f_acc[here, :].astype(BF)
        f_out[here, :] = forget
        v_out[here, :] = v_acc[here, :].astype(BF)
        decay = jnp.sum(jnp.log(1.0 - gates(forget, slack_ref[...])), axis=0, keepdims=True)
        damping = jnp.sum(damp_ref[s], axis=1, keepdims=True)
        for h in range(heads):
            totals.append(decay[:, h * head_dim : (h + 1) * head_dim] + damping[h : h + 1, :])
    totals = jnp.concatenate(totals)
    for p in range(total_ref.shape[0]):
        total_ref[p] = totals


def log_totals(pieces, plan, weights, sums, slack, damp, parts):
    seqs, heads, _ = damp.shape
    return in_vmem(
        functools.partial(total_kernel, plan=plan),
        [jax.ShapeDtypeStruct(s.shape, BF) for s in sums]
        + [jax.ShapeDtypeStruct((parts, seqs * heads, weights[0].shape[1] // heads), F32)],
        *pieces,
        *weights,
        *sums,
        slack,
        damp,
        scratch=[pltpu.VMEM(s.shape, F32) for s in sums],
        flops=12 * len(pieces) * pieces[0].size * weights[0].shape[1],
    )


def state_kernel(forget_ref, value_ref, slack_ref, damp_ref, *refs):
    *outs, state_ref, parts_ref = refs
    far, rows, head_dim = parts_ref.shape[1], *parts_ref.shape[3:]
    seqs, heads, length = damp_ref.shape
    channels = heads * head_dim
    tall = length + 8
    row = lax.broadcasted_iota(jnp.int32, (tall, length), 0)
    column = lax.broadcasted_iota(jnp.int32, (tall, length), 1)
    later = jnp.where((column > row) | (row >= length), 1.0, 0.0).astype(BF)
    head = lax.broadcasted_iota(jnp.int32, (3 * heads, channels), 0) % heads
    channel = lax.broadcasted_iota(jnp.int32, (3 * heads, channels), 1)
    spread = jnp.where(channel // head_dim == head, 1.0, 0.0).astype(BF)
    over_rows = (((0,), (0,)), ((), ()))
    over_columns = (((1,), (1,)), ((), ()))
    totals = []
    for s in range(seqs):
        here = pl.ds(s * length, length)
        values = value_ref[here, :]
        gate = gates(forget_ref[here, :], slack_ref[...])
        high, middle, _ = three_terms(jnp.log(1.0 - gate))
        damping = lax.dot_general(
            later,
            jnp.concatenate(three_terms(damp_ref[s])),
            over_columns,
            preferred_element_type=F32,
        )
        damping = damping[:, :heads] + damping[:, heads : 2 * heads] + damping[:, 2 * heads :]
        sums = jnp.dot(
            jnp.concatenate([later, *three_terms(damping)], axis=1),
            jnp.concatenate([high, spread]),
            preferred_element_type=F32,
        ) + jnp.dot(later, middle, preferred_element_type=F32)
        weighted = (gate * jnp.exp(sums[:length])).astype(BF)
        for h in range(heads):
            cols = slice(h * head_dim, (h + 1) * head_dim)
            state = lax.dot_general(
                weighted[:, cols], values[:, cols], over_rows, preferred_element_type=F32
            )
            totals.append(sums[length : length + 1, cols])
            state = state.astype(BF)
            state_ref[s * heads + h] = state
            blocks = state.reshape(far, NEAR, rows, head_dim)
            for y in range(NEAR):
                parts_ref[y, :, s * heads + h] = blocks[:, y]
    pairs = seqs * heads
    terms = [t.astype(F32) for t in three_terms(jnp.concatenate(totals))]
    packed = jnp.concatenate([*terms, jnp.zeros((head_dim - 3 * pairs, head_dim), F32)])
    blocks = packed.T.astype(BF).reshape(far, NEAR, rows, head_dim)
    for y in range(NEAR):
        parts_ref[y, :, pairs] = blocks[:, y]
    near = lax.rem(lax.axis_index("sp"), NEAR)
    for step, out in enumerate(outs):
        out[...] = parts_ref[near ^ step]


def states(forget, values, slack, damp, parts):
    seqs, heads, _ = damp.shape
    head_dim = forget.shape[1] // heads
    pairs = seqs * heads
    shape = (parts // NEAR, pairs + 1, head_dim // parts, head_dim)
    *outs, state = in_vmem(
        state_kernel,
        [jax.ShapeDtypeStruct(shape, BF)] * NEAR
        + [jax.ShapeDtypeStruct((pairs, head_dim, head_dim), BF)],
        forget,
        values,
        slack,
        damp,
        scratch=[pltpu.VMEM((NEAR, *shape), BF)],
        flops=4 * forget.size * head_dim,
    )
    return outs, state


def unpacked(tile, pairs):
    tile = tile.astype(F32)
    lanes = tile.shape[1]
    return tile + pltpu.roll(tile, lanes - pairs, 1) + pltpu.roll(tile, lanes - 2 * pairs, 1)


def joined(tiles, place):
    pairs = tiles[0].shape[0] - 1
    places = [place ^ step for step in range(len(tiles))]
    totals = [unpacked(tile[pairs], pairs) for tile in tiles]
    sums = [None] * pairs
    for here, tile in zip(places, tiles):
        after = sum(jnp.where(p > here, 1.0, 0.0) * total for p, total in zip(places, totals))
        scale = jnp.exp(after)
        for j in range(pairs):
            part = scale[:, j : j + 1] * tile[j].astype(F32)
            sums[j] = part if sums[j] is None else sums[j] + part
    return sums, sum(totals)


def near_kernel(*refs):
    tiles, outs, parts_ref = refs[:NEAR], refs[NEAR:-1], refs[-1]
    far, tile_count, rows, lanes = parts_ref.shape
    pairs = tile_count - 1
    me = lax.axis_index("sp")
    lane = lax.broadcasted_iota(jnp.int32, (rows, lanes), 1)
    for z in range(far):
        sums, total = joined([t.at[z] for t in tiles], lax.rem(me, NEAR))
        for j in range(pairs):
            parts_ref[z, j] = sums[j].astype(BF)
        high, middle, low = (t.astype(F32) for t in three_terms(total))
        packed = jnp.where(lane < 2 * pairs, pltpu.roll(middle, pairs, 1), pltpu.roll(low, 2 * pairs, 1))
        packed = jnp.where(lane < pairs, high, packed)
        parts_ref[z, pairs] = jnp.where(lane < 3 * pairs, packed, 0.0).astype(BF)
    for step, out in enumerate(outs):
        out[...] = parts_ref[(me // NEAR) ^ step]


def join_near(tiles):
    shape = tiles[0].shape
    return in_vmem(
        near_kernel,
        [jax.ShapeDtypeStruct(shape[1:], BF)] * shape[0],
        *tiles,
        scratch=[pltpu.VMEM(shape, BF)],
    )


def far_kernel(*refs):
    tiles, cache_ref = refs[:-1], refs[-1]
    sums, _ = joined(tiles, lax.axis_index("sp") // NEAR)
    for j, part in enumerate(sums):
        cache_ref[j] = part.astype(BF)


def join_far(tiles):
    tile_count, rows, lanes = tiles[0].shape
    return in_vmem(far_kernel, pltpu.VMEM((tile_count - 1, rows, lanes), BF), *tiles)


def read_kernel(totals_ref, state_ref, query_ref, keys_ref, out_ref):
    me = lax.axis_index("sp")
    after = sum(
        jnp.where(src > me, 1.0, 0.0) * totals_ref[src] for src in range(totals_ref.shape[0])
    )
    weights = query_ref[...] * (1.0 - keys_ref[...]) * jnp.exp(after)
    pairs = weights.shape[0]
    terms = jnp.concatenate(three_terms(weights))
    reads = []
    for j in range(pairs):
        parts = jnp.dot(terms, state_ref[j], preferred_element_type=F32)
        reads.append(sum(parts[n : n + 1, :] for n in range(j, 3 * pairs, pairs)))
    reads = jnp.concatenate(reads)
    for p in range(out_ref.shape[0]):
        out_ref[p] = reads


def read_parts(totals, state, query, keys):
    return in_vmem(read_kernel, jax.ShapeDtypeStruct(totals.shape, F32), totals, state, query, keys)


def finish_kernel(got_ref, query_ref, keys_ref, value_ref, norm_ref, gate_ref, out_ref):
    heads = out_ref.shape[1] // got_ref.shape[2]
    head_dim = got_ref.shape[2]
    shared = jnp.sum(query_ref[...] * keys_ref[...], axis=1, keepdims=True)
    read = shared * value_ref[...]
    for src in range(got_ref.shape[0]):
        read = read + got_ref[src]
    scaled = read * lax.rsqrt(jnp.mean(read * read, axis=1, keepdims=True) + 1e-06) * norm_ref[...]
    result = (scaled * gate_ref[...]).astype(BF)
    for s in range(out_ref.shape[0]):
        for h in range(heads):
            j = s * heads + h
            out_ref[s : s + 1, h * head_dim : (h + 1) * head_dim] = result[j : j + 1, :]


def new_token_kernel(x_ref, q_hbm, g_hbm, f_hbm, v_hbm, out_ref, x_here, rows, sems):
    seqs, slab = x_ref.shape
    here = pl.ds(pl.multiple_of(lax.axis_index("sp") * slab, slab), slab)
    sources = (q_hbm, g_hbm, f_hbm.at[here], v_hbm.at[here])
    copied([(w, rows.at[n]) for n, w in enumerate(sources)] + [(x_ref, x_here)], sems)
    for n in range(len(sources)):
        y = jnp.dot(x_here[...], rows[n], preferred_element_type=F32)
        for p in range(out_ref.shape[0]):
            out_ref[p, n * seqs : (n + 1) * seqs, :] = y


def prepare_kernel(got_ref, slack_ref, query_ref, keys_ref, value_ref, gate_ref):
    pairs, head_dim = value_ref.shape
    seqs = got_ref.shape[1] // 4
    heads = pairs // seqs
    total = got_ref[0]
    for src in range(1, got_ref.shape[0]):
        total = total + got_ref[src]
    rounded = total.astype(BF).astype(F32)

    def by_head(x):
        return jnp.concatenate(
            [
                x[s : s + 1, h * head_dim : (h + 1) * head_dim]
                for s in range(x.shape[0])
                for h in range(heads)
            ]
        )

    query, gate, forget, value = (rounded[n * seqs : (n + 1) * seqs] for n in range(4))
    keys = slack_ref[...] * jax.nn.sigmoid(-forget)
    value_ref[...] = by_head(value)
    gate_ref[...] = by_head(gate * jax.nn.sigmoid(gate))
    query_ref[...] = by_head(query)
    keys_ref[...] = by_head(keys)


def per_device(
    tokens,
    first_token_input,
    forget_weight,
    value_weight,
    query_weight,
    output_gate_weight,
    forget_bound_slack,
    additional_damping_exponent,
    read_norm_scale,
):
    seqs, length, width = tokens.shape
    head_dim = read_norm_scale.shape[0]
    heads = additional_damping_exponent.shape[2]
    channels = heads * head_dim
    sp_count = lax.axis_size("sp")
    tp_count = lax.axis_size("tp")
    chips = tp_count // 2
    slack = forget_bound_slack.reshape(1, channels)

    def shifted(x, by):
        pairs = [(2 * c + k, 2 * ((c + by) % chips) + k) for c in range(chips) for k in (0, 1)]
        return lax.ppermute(x, "tp", pairs)

    def sibling(x):
        return lax.ppermute(x, "tp", [(i, i ^ 1) for i in range(tp_count)])

    def exchange(x):
        return lax.all_to_all(x, "sp", 0, 0, tiled=True)

    rows = seqs // 2 * length
    own = tokens.reshape(seqs * length, width)
    other = sibling(own)
    own_a, own_b = (x.reshape(rows, width) for x in split(tokens, 2))
    right_a, left_a = shifted(own_a, 1), shifted(own_a, -1)
    right_b, left_b = shifted(own_b, 1), shifted(own_b, -1)

    partial = in_vmem(
        new_token_kernel,
        jax.ShapeDtypeStruct((sp_count, 4 * seqs, channels), F32),
        *(
            pltpu.with_memory_space_constraint(x, pltpu.HBM)
            for x in (
                first_token_input,
                query_weight,
                output_gate_weight,
                forget_weight,
                value_weight,
            )
        ),
        in_specs=[pl.BlockSpec(memory_space=pltpu.HBM)] * 5,
        scratch=[
            pltpu.VMEM(first_token_input.shape, BF),
            pltpu.VMEM((4, *query_weight.shape), BF),
            pltpu.SemaphoreType.DMA((5,)),
        ],
    )
    new_sums = exchange(partial)
    row_count = head_dim // sp_count
    pairs = seqs * heads
    query_new, keys_new, value_new, gate_new = in_vmem(
        prepare_kernel, [jax.ShapeDtypeStruct((pairs, head_dim), F32)] * 4, new_sums, slack
    )

    far_a, far_b = shifted(right_a, 1), shifted(left_b, -1)
    other_right_a, other_left_a = sibling(right_a), sibling(left_a)
    other_right_b, other_left_b = sibling(right_b), sibling(left_b)
    other_far_a, other_far_b = sibling(far_a), sibling(far_b)

    def both(by):
        return ((by, False), (by, True))

    weights, sums = load_and_project(
        own, other, (both(0),), (forget_weight, value_weight)
    )
    pieces = [right_a, other_right_a, left_b, other_left_b]
    sums = project(pieces, (both(1), both(-1)), weights, sums)
    pieces = [left_a, other_left_a, right_b, other_right_b]
    sums = project(pieces, (both(-1), both(1)), weights, sums)
    sums = project([far_a, far_b], (((2, False),), ((2, False),)), weights, sums)
    damp = additional_damping_exponent.transpose(0, 2, 1)
    forget, values, totals = log_totals(
        [other_far_a, other_far_b],
        (((2, True),), ((2, True),)),
        weights,
        sums,
        slack,
        damp,
        sp_count,
    )
    parts, state = states(forget, values, slack, damp, sp_count)

    planes = sp_count // NEAR

    def along_y(step):
        pairs = [
            (z * NEAR + y, z * NEAR + (y ^ step)) for z in range(planes) for y in range(NEAR)
        ]
        return lax.ppermute(parts[step], "sp", pairs)

    def along_z(step):
        pairs = [
            (z * NEAR + y, (z ^ step) * NEAR + y)
            for z in range(planes)
            for y in range(NEAR)
        ]
        return lax.ppermute(parts[step], "sp", pairs)

    parts = [parts[0], *(along_y(step) for step in range(1, NEAR))]
    parts = join_near(parts)
    parts = [parts[0], *(along_z(step) for step in range(1, planes))]
    cache = join_far(parts)

    totals = exchange(totals)
    read = read_parts(totals, state, query_new, keys_new)
    got = exchange(read)
    first_read = in_vmem(
        finish_kernel,
        jax.ShapeDtypeStruct((seqs, channels), BF),
        got,
        query_new,
        keys_new,
        value_new,
        read_norm_scale.reshape(1, head_dim),
        gate_new,
    )
    return cache.reshape(seqs, heads, row_count, head_dim), first_read


def solution(mesh):
    placed = (
        P("gr", "sp", "tp"),
        P("gr", "sp"),
        P(None, "tp"),
        P(None, "tp"),
        P("sp", "tp"),
        P("sp", "tp"),
        P("tp"),
        P("gr", "sp", "tp"),
        P(),
    )

    return jax.shard_map(
        per_device,
        mesh=mesh,
        in_specs=placed,
        out_specs=(P("gr", "tp", "sp", None), P("gr", "tp")),
        check_vma=False,
    )
```

```python
import functools

import jax
import jax.numpy as jnp
from jax import lax
from jax.experimental import pallas as pl
from jax.experimental.pallas import tpu as pltpu
from jax.sharding import PartitionSpec as P


BF = jnp.bfloat16
F32 = jnp.float32
NEAR = 4


def three_terms(x):
    high = x.astype(BF)
    rest = x - high.astype(F32)
    middle = rest.astype(BF)
    low = (rest - middle.astype(F32)).astype(BF)
    return high, middle, low


VMEM = pl.BlockSpec(memory_space=pltpu.VMEM)


def in_vmem(kernel, out_shape, *arrays, in_specs=None, scratch=(), flops=0):
    return pl.pallas_call(
        kernel,
        in_specs=in_specs or [VMEM] * len(arrays),
        out_specs=jax.tree.map(lambda _: VMEM, out_shape),
        out_shape=out_shape,
        scratch_shapes=scratch,
        compiler_params=pltpu.CompilerParams(vmem_limit_bytes=12 << 20),
        cost_estimate=pl.CostEstimate(flops=flops, transcendentals=0, bytes_accessed=0),
    )(*arrays)


def copied(pairs, sems):
    copies = [pltpu.make_async_copy(*pair, sems.at[n]) for n, pair in enumerate(pairs)]
    for copy in copies:
        copy.start()
    for copy in copies:
        copy.wait()


def from_hbm(kernel, shapes, *arrays):
    return pl.pallas_call(
        kernel,
        in_specs=[pl.BlockSpec(memory_space=pltpu.HBM)] * len(arrays),
        out_specs=[VMEM] * len(shapes),
        out_shape=[pltpu.VMEM(shape, BF) for shape in shapes],
        scratch_shapes=[pltpu.SemaphoreType.DMA((len(shapes),))],
        compiler_params=pltpu.CompilerParams(vmem_limit_bytes=1 << 20),
    )(*(pltpu.with_memory_space_constraint(a, pltpu.HBM) for a in arrays))


def split_kernel(tokens_ref, *refs):
    seqs = tokens_ref.shape[0] // (len(refs) - 1)
    copied(
        [(tokens_ref.at[pl.ds(n * seqs, seqs)], out) for n, out in enumerate(refs[:-1])], refs[-1]
    )


def split(tokens, count):
    shape = (tokens.shape[0] // count, *tokens.shape[1:])
    return from_hbm(split_kernel, [shape] * count, tokens)


def block_of(tp, by, other):
    count = lax.axis_size("tp")
    return lax.rem((tp ^ 1 if other else tp) + count - 2 * by, count)


def products(pieces, sources, w_ref):
    tp = lax.axis_index("tp")
    total = None
    for piece, source in zip(pieces, sources):
        width = piece.shape[1]
        start = pl.multiple_of(block_of(tp, *source) * width, width)
        part = jnp.dot(piece[...], w_ref[pl.ds(start, width), :], preferred_element_type=F32)
        total = part if total is None else total + part
    return total


def add_products(pieces, plan, weights, sums, outs):
    rows = pieces[0].shape[0]
    for half, sources in enumerate(plan):
        here = pl.ds(half * rows, rows)
        some, pieces = pieces[: len(sources)], pieces[len(sources) :]
        for n, (w_ref, out) in enumerate(zip(weights, outs)):
            result = products(some, sources, w_ref)
            out[here, :] = sums[n][here, :] + result if sums else result


def project_kernel(*refs, plan):
    count = sum(map(len, plan))
    add_products(refs[:count], plan, refs[count : count + 2], refs[-4:-2], refs[-2:])


def project(pieces, plan, weights, sums):
    return in_vmem(
        functools.partial(project_kernel, plan=plan),
        [jax.ShapeDtypeStruct(s.shape, F32) for s in sums],
        *pieces,
        *weights,
        *sums,
        flops=4 * len(pieces) * pieces[0].size * weights[0].shape[1],
    )


def load_kernel(own_hbm, other_hbm, wf_hbm, wv_hbm, *refs, plan):
    wf_ref, wv_ref, *outs, own_ref, other_ref, sems = refs
    chips = lax.axis_size("tp") // 2
    depth = wf_ref.shape[0] // chips
    chip = lax.axis_index("tp") // 2
    pairs = [(own_hbm, own_ref), (other_hbm, other_ref)]
    for step in range(chips):
        here = pl.ds(pl.multiple_of(lax.rem(chip + step, chips) * depth, depth), depth)
        pairs += [(wf_hbm.at[here], wf_ref.at[here]), (wv_hbm.at[here], wv_ref.at[here])]
    copies = [pltpu.make_async_copy(*pair, sems.at[n]) for n, pair in enumerate(pairs)]
    for copy in copies:
        copy.start()
    for copy in copies[:4]:
        copy.wait()
    add_products((own_ref, other_ref), plan, (wf_ref, wv_ref), (), outs)
    for copy in copies[4:]:
        copy.wait()


def load_and_project(own, other, plan, weights):
    out = jax.ShapeDtypeStruct((own.shape[0], weights[0].shape[1]), F32)
    *weights, f, v = pl.pallas_call(
        functools.partial(load_kernel, plan=plan),
        in_specs=[pl.BlockSpec(memory_space=pltpu.HBM)] * 4,
        out_specs=[VMEM] * 4,
        out_shape=[pltpu.VMEM(w.shape, BF) for w in weights] + [out] * 2,
        scratch_shapes=[pltpu.VMEM(own.shape, BF)] * 2
        + [pltpu.SemaphoreType.DMA((lax.axis_size("tp") + 2,))],
        compiler_params=pltpu.CompilerParams(vmem_limit_bytes=12 << 20),
        name="load",
    )(*(pltpu.with_memory_space_constraint(x, pltpu.HBM) for x in (own, other, *weights)))
    return [pltpu.with_memory_space_constraint(w, pltpu.VMEM) for w in weights], [f, v]


def gates(forget, slack):
    return slack / (1.0 + jnp.exp(forget.astype(F32)))


def total_kernel(*refs, plan):
    count = sum(map(len, plan))
    pieces, (wf_ref, wv_ref, f_in, v_in, *refs) = refs[:count], refs[count:]
    slack_ref, damp_ref, f_out, v_out, total_ref, f_acc, v_acc = refs
    add_products(pieces, plan, (wf_ref, wv_ref), (f_in, v_in), (f_acc, v_acc))
    seqs, heads, length = damp_ref.shape
    head_dim = total_ref.shape[2]
    totals = []
    for s in range(seqs):
        here = pl.ds(s * length, length)
        forget = f_acc[here, :].astype(BF)
        f_out[here, :] = forget
        v_out[here, :] = v_acc[here, :].astype(BF)
        decay = jnp.sum(jnp.log(1.0 - gates(forget, slack_ref[...])), axis=0, keepdims=True)
        damping = jnp.sum(damp_ref[s], axis=1, keepdims=True)
        for h in range(heads):
            totals.append(decay[:, h * head_dim : (h + 1) * head_dim] + damping[h : h + 1, :])
    totals = jnp.concatenate(totals)
    for p in range(total_ref.shape[0]):
        total_ref[p] = totals


def log_totals(pieces, plan, weights, sums, slack, damp, parts):
    seqs, heads, _ = damp.shape
    return in_vmem(
        functools.partial(total_kernel, plan=plan),
        [jax.ShapeDtypeStruct(s.shape, BF) for s in sums]
        + [jax.ShapeDtypeStruct((parts, seqs * heads, weights[0].shape[1] // heads), F32)],
        *pieces,
        *weights,
        *sums,
        slack,
        damp,
        scratch=[pltpu.VMEM(s.shape, F32) for s in sums],
        flops=12 * len(pieces) * pieces[0].size * weights[0].shape[1],
    )


def state_kernel(forget_ref, value_ref, slack_ref, damp_ref, *refs):
    *outs, state_ref, parts_ref = refs
    far, rows, head_dim = parts_ref.shape[1], *parts_ref.shape[3:]
    seqs, heads, length = damp_ref.shape
    channels = heads * head_dim
    tall = length + 8
    row = lax.broadcasted_iota(jnp.int32, (tall, length), 0)
    column = lax.broadcasted_iota(jnp.int32, (tall, length), 1)
    later = jnp.where((column > row) | (row >= length), 1.0, 0.0).astype(BF)
    head = lax.broadcasted_iota(jnp.int32, (3 * heads, channels), 0) % heads
    channel = lax.broadcasted_iota(jnp.int32, (3 * heads, channels), 1)
    spread = jnp.where(channel // head_dim == head, 1.0, 0.0).astype(BF)
    over_rows = (((0,), (0,)), ((), ()))
    over_columns = (((1,), (1,)), ((), ()))
    totals = []
    for s in range(seqs):
        here = pl.ds(s * length, length)
        values = value_ref[here, :]
        gate = gates(forget_ref[here, :], slack_ref[...])
        high, middle, _ = three_terms(jnp.log(1.0 - gate))
        damping = lax.dot_general(
            later,
            jnp.concatenate(three_terms(damp_ref[s])),
            over_columns,
            preferred_element_type=F32,
        )
        damping = damping[:, :heads] + damping[:, heads : 2 * heads] + damping[:, 2 * heads :]
        sums = jnp.dot(
            jnp.concatenate([later, *three_terms(damping)], axis=1),
            jnp.concatenate([high, spread]),
            preferred_element_type=F32,
        ) + jnp.dot(later, middle, preferred_element_type=F32)
        weighted = (gate * jnp.exp(sums[:length])).astype(BF)
        for h in range(heads):
            cols = slice(h * head_dim, (h + 1) * head_dim)
            state = lax.dot_general(
                weighted[:, cols], values[:, cols], over_rows, preferred_element_type=F32
            )
            totals.append(sums[length : length + 1, cols])
            state = state.astype(BF)
            state_ref[s * heads + h] = state
            blocks = state.reshape(far, NEAR, rows, head_dim)
            for y in range(NEAR):
                parts_ref[y, :, s * heads + h] = blocks[:, y]
    pairs = seqs * heads
    terms = [t.astype(F32) for t in three_terms(jnp.concatenate(totals))]
    packed = jnp.concatenate([*terms, jnp.zeros((head_dim - 3 * pairs, head_dim), F32)])
    blocks = packed.T.astype(BF).reshape(far, NEAR, rows, head_dim)
    for y in range(NEAR):
        parts_ref[y, :, pairs] = blocks[:, y]
    near = lax.rem(lax.axis_index("sp"), NEAR)
    for step, out in enumerate(outs):
        out[...] = parts_ref[near ^ step]


def states(forget, values, slack, damp, parts):
    seqs, heads, _ = damp.shape
    head_dim = forget.shape[1] // heads
    pairs = seqs * heads
    shape = (parts // NEAR, pairs + 1, head_dim // parts, head_dim)
    *outs, state = in_vmem(
        state_kernel,
        [jax.ShapeDtypeStruct(shape, BF)] * NEAR
        + [jax.ShapeDtypeStruct((pairs, head_dim, head_dim), BF)],
        forget,
        values,
        slack,
        damp,
        scratch=[pltpu.VMEM((NEAR, *shape), BF)],
        flops=4 * forget.size * head_dim,
    )
    return outs, state


def unpacked(tile, pairs):
    tile = tile.astype(F32)
    lanes = tile.shape[1]
    return tile + pltpu.roll(tile, lanes - pairs, 1) + pltpu.roll(tile, lanes - 2 * pairs, 1)


def joined(tiles, place):
    pairs = tiles[0].shape[0] - 1
    places = [place ^ step for step in range(len(tiles))]
    totals = [unpacked(tile[pairs], pairs) for tile in tiles]
    sums = [None] * pairs
    for here, tile in zip(places, tiles):
        after = sum(jnp.where(p > here, 1.0, 0.0) * total for p, total in zip(places, totals))
        scale = jnp.exp(after)
        for j in range(pairs):
            part = scale[:, j : j + 1] * tile[j].astype(F32)
            sums[j] = part if sums[j] is None else sums[j] + part
    return sums, sum(totals)


def near_kernel(*refs):
    tiles, outs, parts_ref = refs[:NEAR], refs[NEAR:-1], refs[-1]
    far, tile_count, rows, lanes = parts_ref.shape
    pairs = tile_count - 1
    me = lax.axis_index("sp")
    lane = lax.broadcasted_iota(jnp.int32, (rows, lanes), 1)
    for z in range(far):
        sums, total = joined([t.at[z] for t in tiles], lax.rem(me, NEAR))
        for j in range(pairs):
            parts_ref[z, j] = sums[j].astype(BF)
        high, middle, low = (t.astype(F32) for t in three_terms(total))
        packed = jnp.where(lane < 2 * pairs, pltpu.roll(middle, pairs, 1), pltpu.roll(low, 2 * pairs, 1))
        packed = jnp.where(lane < pairs, high, packed)
        parts_ref[z, pairs] = jnp.where(lane < 3 * pairs, packed, 0.0).astype(BF)
    for step, out in enumerate(outs):
        out[...] = parts_ref[(me // NEAR) ^ step]


def join_near(tiles):
    shape = tiles[0].shape
    return in_vmem(
        near_kernel,
        [jax.ShapeDtypeStruct(shape[1:], BF)] * shape[0],
        *tiles,
        scratch=[pltpu.VMEM(shape, BF)],
    )


def read_kernel(totals_ref, state_ref, query_ref, keys_ref, out_ref):
    me = lax.axis_index("sp")
    after = sum(
        jnp.where(src > me, 1.0, 0.0) * totals_ref[src] for src in range(totals_ref.shape[0])
    )
    weights = query_ref[...] * (1.0 - keys_ref[...]) * jnp.exp(after)
    pairs = weights.shape[0]
    terms = jnp.concatenate(three_terms(weights))
    reads = []
    for j in range(pairs):
        parts = jnp.dot(terms, state_ref[j], preferred_element_type=F32)
        reads.append(sum(parts[n : n + 1, :] for n in range(j, 3 * pairs, pairs)))
    reads = jnp.concatenate(reads)
    for p in range(out_ref.shape[0]):
        out_ref[p] = reads


def read_parts(totals, state, query, keys):
    return in_vmem(read_kernel, jax.ShapeDtypeStruct(totals.shape, F32), totals, state, query, keys)


def finish_kernel(
    got_ref, query_ref, keys_ref, value_ref, norm_ref, gate_ref, *refs
):
    *tiles, cache_ref, out_ref = refs
    sums, _ = joined(tiles, lax.axis_index("sp") // NEAR)
    for j, part in enumerate(sums):
        cache_ref[j] = part.astype(BF)
    heads = out_ref.shape[1] // got_ref.shape[2]
    head_dim = got_ref.shape[2]
    shared = jnp.sum(query_ref[...] * keys_ref[...], axis=1, keepdims=True)
    read = shared * value_ref[...]
    for src in range(got_ref.shape[0]):
        read = read + got_ref[src]
    scaled = read * lax.rsqrt(jnp.mean(read * read, axis=1, keepdims=True) + 1e-06) * norm_ref[...]
    result = (scaled * gate_ref[...]).astype(BF)
    for s in range(out_ref.shape[0]):
        for h in range(heads):
            j = s * heads + h
            out_ref[s : s + 1, h * head_dim : (h + 1) * head_dim] = result[j : j + 1, :]


def new_token_kernel(x_ref, q_hbm, g_hbm, f_hbm, v_hbm, out_ref, x_here, rows, sems):
    seqs, slab = x_ref.shape
    here = pl.ds(pl.multiple_of(lax.axis_index("sp") * slab, slab), slab)
    sources = (q_hbm, g_hbm, f_hbm.at[here], v_hbm.at[here])
    copied([(w, rows.at[n]) for n, w in enumerate(sources)] + [(x_ref, x_here)], sems)
    for n in range(len(sources)):
        y = jnp.dot(x_here[...], rows[n], preferred_element_type=F32)
        for p in range(out_ref.shape[0]):
            out_ref[p, n * seqs : (n + 1) * seqs, :] = y


def prepare_kernel(got_ref, slack_ref, query_ref, keys_ref, value_ref, gate_ref):
    pairs, head_dim = value_ref.shape
    seqs = got_ref.shape[1] // 4
    heads = pairs // seqs
    total = got_ref[0]
    for src in range(1, got_ref.shape[0]):
        total = total + got_ref[src]
    rounded = total.astype(BF).astype(F32)

    def by_head(x):
        return jnp.concatenate(
            [
                x[s : s + 1, h * head_dim : (h + 1) * head_dim]
                for s in range(x.shape[0])
                for h in range(heads)
            ]
        )

    query, gate, forget, value = (rounded[n * seqs : (n + 1) * seqs] for n in range(4))
    keys = slack_ref[...] * jax.nn.sigmoid(-forget)
    value_ref[...] = by_head(value)
    gate_ref[...] = by_head(gate * jax.nn.sigmoid(gate))
    query_ref[...] = by_head(query)
    keys_ref[...] = by_head(keys)


def per_device(
    tokens,
    first_token_input,
    forget_weight,
    value_weight,
    query_weight,
    output_gate_weight,
    forget_bound_slack,
    additional_damping_exponent,
    read_norm_scale,
):
    seqs, length, width = tokens.shape
    head_dim = read_norm_scale.shape[0]
    heads = additional_damping_exponent.shape[2]
    channels = heads * head_dim
    sp_count = lax.axis_size("sp")
    tp_count = lax.axis_size("tp")
    chips = tp_count // 2
    slack = forget_bound_slack.reshape(1, channels)

    def shifted(x, by):
        pairs = [(2 * c + k, 2 * ((c + by) % chips) + k) for c in range(chips) for k in (0, 1)]
        return lax.ppermute(x, "tp", pairs)

    def sibling(x):
        return lax.ppermute(x, "tp", [(i, i ^ 1) for i in range(tp_count)])

    def exchange(x):
        return lax.all_to_all(x, "sp", 0, 0, tiled=True)

    rows = seqs // 2 * length
    own = tokens.reshape(seqs * length, width)
    other = sibling(own)
    own_a, own_b = (x.reshape(rows, width) for x in split(tokens, 2))
    right_a, left_a = shifted(own_a, 1), shifted(own_a, -1)
    right_b, left_b = shifted(own_b, 1), shifted(own_b, -1)

    partial = in_vmem(
        new_token_kernel,
        jax.ShapeDtypeStruct((sp_count, 4 * seqs, channels), F32),
        *(
            pltpu.with_memory_space_constraint(x, pltpu.HBM)
            for x in (
                first_token_input,
                query_weight,
                output_gate_weight,
                forget_weight,
                value_weight,
            )
        ),
        in_specs=[pl.BlockSpec(memory_space=pltpu.HBM)] * 5,
        scratch=[
            pltpu.VMEM(first_token_input.shape, BF),
            pltpu.VMEM((4, *query_weight.shape), BF),
            pltpu.SemaphoreType.DMA((5,)),
        ],
    )
    new_sums = exchange(partial)
    row_count = head_dim // sp_count
    pairs = seqs * heads
    query_new, keys_new, value_new, gate_new = in_vmem(
        prepare_kernel, [jax.ShapeDtypeStruct((pairs, head_dim), F32)] * 4, new_sums, slack
    )

    far_a, far_b = shifted(right_a, 1), shifted(left_b, -1)
    other_right_a, other_left_a = sibling(right_a), sibling(left_a)
    other_right_b, other_left_b = sibling(right_b), sibling(left_b)
    other_far_a, other_far_b = sibling(far_a), sibling(far_b)

    def both(by):
        return ((by, False), (by, True))

    weights, sums = load_and_project(
        own, other, (both(0),), (forget_weight, value_weight)
    )
    pieces = [right_a, other_right_a, left_b, other_left_b]
    sums = project(pieces, (both(1), both(-1)), weights, sums)
    pieces = [left_a, other_left_a, right_b, other_right_b]
    sums = project(pieces, (both(-1), both(1)), weights, sums)
    sums = project([far_a, far_b], (((2, False),), ((2, False),)), weights, sums)
    damp = additional_damping_exponent.transpose(0, 2, 1)
    forget, values, totals = log_totals(
        [other_far_a, other_far_b],
        (((2, True),), ((2, True),)),
        weights,
        sums,
        slack,
        damp,
        sp_count,
    )
    parts, state = states(forget, values, slack, damp, sp_count)

    planes = sp_count // NEAR

    def along_y(step):
        pairs = [
            (z * NEAR + y, z * NEAR + (y ^ step)) for z in range(planes) for y in range(NEAR)
        ]
        return lax.ppermute(parts[step], "sp", pairs)

    def along_z(step):
        pairs = [
            (z * NEAR + y, (z ^ step) * NEAR + y)
            for z in range(planes)
            for y in range(NEAR)
        ]
        return lax.ppermute(parts[step], "sp", pairs)

    parts = [parts[0], *(along_y(step) for step in range(1, NEAR))]
    parts = join_near(parts)
    parts = [parts[0], *(along_z(step) for step in range(1, planes))]

    totals = exchange(totals)
    read = read_parts(totals, state, query_new, keys_new)
    got = exchange(read)
    cache, first_read = in_vmem(
        finish_kernel,
        [
            jax.ShapeDtypeStruct((pairs, row_count, head_dim), BF),
            jax.ShapeDtypeStruct((seqs, channels), BF),
        ],
        got,
        query_new,
        keys_new,
        value_new,
        read_norm_scale.reshape(1, head_dim),
        gate_new,
        *parts,
    )
    return cache.reshape(seqs, heads, row_count, head_dim), first_read


def solution(mesh):
    placed = (
        P("gr", "sp", "tp"),
        P("gr", "sp"),
        P(None, "tp"),
        P(None, "tp"),
        P("sp", "tp"),
        P("sp", "tp"),
        P("tp"),
        P("gr", "sp", "tp"),
        P(),
    )

    return jax.shard_map(
        per_device,
        mesh=mesh,
        in_specs=placed,
        out_specs=(P("gr", "tp", "sp", None), P("gr", "tp")),
        check_vma=False,
    )
```
